128 devices in a mesh: sp: 32 (over z, y, core), tp: 4 (over x).
Axes of the slice: x: 4, y: 4, z: 4, core: 2. Of those that a mesh axis runs over, the one named last changes fastest.
Arguments:
- tokens: bfloat16 [12288, 2048], P('sp', 'tp'), may hold values from -6 to 6
- norm_gain: float32 [2048], replicated, may hold values from 0.1 to 1.9
- w_query_down: bfloat16 [2048, 512], replicated, may hold values from -0.125 to 0.125
- query_gain: float32 [512], replicated, may hold values from 0.1 to 1.9
- w_query_up: bfloat16 [512, 1536], P(None, 'tp'), may hold values from -0.25 to 0.25
- w_latent_down: bfloat16 [2048, 256], replicated, may hold values from -0.125 to 0.125
- latent_gain: float32 [256], replicated, may hold values from 0.1 to 1.9
- w_rotary_key: bfloat16 [2048, 32], replicated, may hold values from -0.125 to 0.125
- w_latent_up: bfloat16 [256, 2048], P(None, 'tp'), may hold values from -0.375 to 0.375
- query_head_gain: float32 [96], replicated, may hold values from 0.1 to 1.9
- key_head_gain: float32 [96], replicated, may hold values from 0.1 to 1.9
- w_pool_in: bfloat16 [2048, 1024], P(None, 'tp'), may hold values from -0.125 to 0.125
- w_pool_mix: bfloat16 [4, 256, 256], P('tp'), may hold values from -0.375 to 0.375
- pool_scale: float32 [1024], P('tp'), may hold values from 0.1 to 1.9
- w_attn_out: bfloat16 [1024, 2048], P('tp'), may hold values from -12 to 12
- w_pool_out: bfloat16 [1024, 2048], P('tp'), may hold values from -0.5 to 0.5
- w_gate_attn: bfloat16 [2048, 2048], P(None, 'tp'), may hold values from -0.125 to 0.125
- w_gate_pool: bfloat16 [2048, 2048], P(None, 'tp'), may hold values from -0.125 to 0.125
Outputs:
- mixed: bfloat16 [12288, 2048], P('sp', 'tp')
The draws below stay inside these ranges and needn't reach their ends.
All inputs are finite; a program needn't handle non-finite values.
Results may differ from the reference program's by a relative error of at most 0.02.
Values may be sent and summed in bfloat16 or wider, within the bound.
A program may use at most 128 MiB of HBM per device.

```python
import math
import jax
import jax.numpy as jnp
from jax import lax

D = 2048
HEADS = 16
QUERY_RANK = 512
LATENT_RANK = 256
NOPE = 64
ROPE = 32
VALUE_DIM = 64
POOL_GROUPS = 4
POOL_GROUP = 256
POOL_WIDTH = 1024
TOKENS = 12288


def level_of(rng, extent, pieces, smallest, top_value):
    def one(dim, shards_of):
        steps = jax.random.uniform(jax.random.fold_in(jax.random.fold_in(rng, 6), dim), (shards_of,), jnp.float32, smallest / len(pieces), top_value / len(pieces))
        return jnp.repeat(jnp.exp(steps), extent[dim] // shards_of).reshape((-1,) + (1,) * (len(extent) - dim - 1))

    level = one(*pieces[0])
    for cut in pieces[1:]:
        level = level * one(*cut)
    return level


def centred(own_key, shape, deviation, most, split=(), held_as=jnp.bfloat16):
    result = jax.random.normal(own_key, shape, jnp.float32) * deviation
    if len(split) > 0:
        result = level_of(own_key, shape, split, -0.22, 0.18) * result
    return jnp.clip(result, min=-most, max=most).astype(held_as)


def setup_inputs(seed: int = 0) -> dict:
    streams_of = jax.random.split(jax.random.key(seed), 19)
    return {
        "tokens": centred(streams_of[0], (TOKENS, D), 1.0, 6.0, ((0, 32), (1, 4))),
        "norm_gain": jnp.clip(1.0 + 0.18 * jax.random.normal(streams_of[1], (D,), jnp.float32), 0.1, 1.9),
        "w_query_down": centred(streams_of[2], (D, QUERY_RANK), D ** -0.5, 0.125),
        "query_gain": jnp.clip(1.0 + 0.18 * jax.random.normal(streams_of[3], (QUERY_RANK,), jnp.float32), 0.1, 1.9),
        "w_query_up": centred(streams_of[4], (QUERY_RANK, HEADS * (NOPE + ROPE)), QUERY_RANK ** -0.5, 0.25, ((1, 4),)),
        "w_latent_down": centred(streams_of[5], (D, LATENT_RANK), D ** -0.5, 0.125),
        "latent_gain": jnp.clip(1.0 + 0.18 * jax.random.normal(streams_of[6], (LATENT_RANK,), jnp.float32), 0.1, 1.9),
        "w_rotary_key": centred(streams_of[7], (D, ROPE), D ** -0.5, 0.125),
        "w_latent_up": centred(streams_of[8], (LATENT_RANK, HEADS * (NOPE + VALUE_DIM)), LATENT_RANK ** -0.5, 0.375, ((1, 4),)),
        "query_head_gain": jnp.clip(1.0 + 0.18 * jax.random.normal(streams_of[9], (NOPE + ROPE,), jnp.float32), 0.1, 1.9),
        "key_head_gain": jnp.clip(1.0 + 0.18 * jax.random.normal(streams_of[10], (NOPE + ROPE,), jnp.float32), 0.1, 1.9),
        "w_pool_in": centred(streams_of[11], (D, POOL_WIDTH), D ** -0.5, 0.125, ((1, 4),)),
        "w_pool_mix": centred(streams_of[12], (POOL_GROUPS, POOL_GROUP, POOL_GROUP), POOL_GROUP ** -0.5, 0.375, ((0, 4),)),
        "pool_scale": jnp.clip(1.0 + 0.18 * jax.random.normal(streams_of[13], (POOL_WIDTH,), jnp.float32), 0.1, 1.9),
        "w_attn_out": centred(streams_of[14], (HEADS * VALUE_DIM, D), 2.0, 12.0, ((0, 4),)),
        "w_pool_out": centred(streams_of[15], (POOL_WIDTH, D), (POOL_WIDTH // 8) ** -0.5, 0.5, ((0, 4),)),
        "w_gate_attn": centred(streams_of[16], (D, D), D ** -0.5, 0.125, ((1, 4),)),
        "w_gate_pool": centred(streams_of[17], (D, D), D ** -0.5, 0.125, ((1, 4),)),
    }


eps = 1e-06
theta = 10000.0

def rms_scale(values, gain):
    values = values.astype(jnp.float32)
    return values * lax.rsqrt(lax.optimization_barrier(jnp.mean(values * values, axis=-1, keepdims=True)) + eps) * gain

def rotate(values, positions):
    half = values.shape[-1] // 2
    freqs = theta ** (-jnp.arange(half, dtype=jnp.float32) / half)
    angles = positions.astype(jnp.float32)[:, None] * freqs[None, :]
    cosine = jnp.cos(angles)[:, None, :]
    sine = jnp.sin(angles)[:, None, :]
    first = values[..., :half]
    second = values[..., half:]
    return jnp.concatenate([first * cosine - second * sine, first * sine + second * cosine], axis=-1)

def head_finish(values, gain, positions):
    normed = rms_scale(values, gain)
    return jnp.concatenate([normed[..., :NOPE], rotate(normed[..., NOPE:], positions)], axis=-1)

def reference(tokens, norm_gain, w_query_down, query_gain, w_query_up, w_latent_down, latent_gain, w_rotary_key, w_latent_up, query_head_gain, key_head_gain, w_pool_in, w_pool_mix, pool_scale, w_attn_out, w_pool_out, w_gate_attn, w_gate_pool):
    length = tokens.shape[0]
    bf = jnp.bfloat16
    positions = jnp.arange(length, dtype=jnp.int32)
    normed = rms_scale(tokens, norm_gain).astype(bf)
    query_latent = jnp.dot(normed, w_query_down, preferred_element_type=jnp.float32).astype(bf)
    query_normed = rms_scale(query_latent, query_gain).astype(bf)
    query_raw = jnp.dot(query_normed, w_query_up, preferred_element_type=jnp.float32).astype(bf)
    query_raw = query_raw.reshape(length, HEADS, NOPE + ROPE)
    query = (head_finish(query_raw, query_head_gain, positions) * (NOPE + ROPE) ** (-0.5)).astype(bf)
    latent = jnp.dot(normed, w_latent_down, preferred_element_type=jnp.float32).astype(bf)
    key_latent = rms_scale(latent, latent_gain).astype(bf)
    rotary_key = jnp.dot(normed, w_rotary_key, preferred_element_type=jnp.float32).astype(bf)
    keys_values = jnp.dot(key_latent, w_latent_up, preferred_element_type=jnp.float32).astype(bf)
    keys_values = keys_values.reshape(length, HEADS, NOPE + VALUE_DIM)
    key_raw = jnp.concatenate([keys_values[..., :NOPE], jnp.broadcast_to(rotary_key[:, None, :], (length, HEADS, ROPE))], axis=-1)
    key = head_finish(key_raw, key_head_gain, positions).astype(bf).astype(jnp.float32)
    values = keys_values[..., NOPE:].astype(jnp.float32)
    block = math.gcd(length, 256)
    query_blocks = query.reshape(length // block, block, HEADS, NOPE + ROPE)

    def attend(query_block):
        scores = jnp.einsum('qhd,khd->hqk', query_block.astype(jnp.float32), key)
        top = lax.optimization_barrier(jnp.max(scores, axis=-1, keepdims=True))
        expo = jnp.exp(scores - top)
        total = lax.optimization_barrier(jnp.sum(expo, axis=-1))
        rounded = lax.optimization_barrier(expo.astype(bf)).astype(jnp.float32)
        weighted = jnp.einsum('hqk,khv->qhv', rounded, values)
        return (weighted / jnp.transpose(total)[:, :, None]).astype(bf)
    attn_rows = lax.map(attend, query_blocks).reshape(length, HEADS * VALUE_DIM)
    pool_input = jnp.dot(normed, w_pool_in, preferred_element_type=jnp.float32).astype(bf)
    reach = 2 ** POOL_GROUPS // 2
    padded = jnp.pad(pool_input.astype(jnp.float32), ((reach, reach), (0, 0)))
    windows = jnp.power(2, jnp.arange(POOL_GROUPS, dtype=jnp.int32) + 1)
    channel_window = jnp.repeat(windows, POOL_GROUP)
    total = jnp.zeros((length, POOL_GROUPS * POOL_GROUP), jnp.float32)
    for shift in range(-reach, reach):
        inside = (shift >= -(channel_window // 2)) & (shift <= channel_window - channel_window // 2 - 1)
        total = total + jnp.where(inside[None, :], padded[reach + shift:reach + shift + length], 0.0)
    low = jnp.clip(positions[:, None] - channel_window[None, :] // 2, 0, length)
    high = jnp.clip(positions[:, None] + channel_window[None, :] - channel_window[None, :] // 2, 0, length)
    count = (high - low).astype(jnp.float32)
    pool_mixed = (total / count - pool_input.astype(jnp.float32)).astype(bf)
    pool_mixed = pool_mixed.reshape(length, POOL_GROUPS, POOL_GROUP)
    grouped = jnp.einsum('lgc,gcd->lgd', pool_mixed.astype(jnp.float32), w_pool_mix.astype(jnp.float32))
    pool_rows = (grouped.reshape(length, POOL_GROUPS * POOL_GROUP) * pool_scale).astype(bf)
    attn_branch = jnp.dot(attn_rows, w_attn_out, preferred_element_type=jnp.float32)
    pool_branch = jnp.dot(pool_rows, w_pool_out, preferred_element_type=jnp.float32)
    gate_attn = jax.nn.sigmoid(jnp.dot(normed, w_gate_attn, preferred_element_type=jnp.float32))
    gate_pool = jax.nn.sigmoid(jnp.dot(normed, w_gate_pool, preferred_element_type=jnp.float32))
    return (gate_attn * attn_branch + gate_pool * pool_branch).astype(bf)
```

```python
import functools
import numpy as np
import jax
import jax.numpy as jnp
from jax import lax
from jax.experimental import pallas as pl
from jax.experimental.pallas import tpu as pltpu
from jax.sharding import PartitionSpec as P

NOPE = 64
ROPE = 32
HEAD = NOPE + ROPE
VALUE_DIM = 64
POOL_GROUPS = 4
POOL_GROUP = 256
ROWS = 384
HEADS_HERE = 4
LATENT = 256
KEY_ROWS = 304
CHUNK = 128
MESH = pl.DeviceIdType.MESH

eps = 1e-06
theta = 10000.0
LOG2E = 1.4426950408889634
bf = jnp.bfloat16
f32 = jnp.float32


def rope_tables():
    half = ROPE // 2
    freqs = theta ** (-np.arange(half, dtype=np.float64) / half)
    fine = np.arange(ROWS)[None, :] * freqs[:, None]
    coarse = (np.arange(128) * ROWS)[None, :] * freqs[:, None]
    fine = np.stack([np.cos(fine), np.sin(fine)]).astype(np.float32)
    coarse = np.stack([np.cos(coarse), np.sin(coarse)]).astype(np.float32)
    return fine, coarse


def column(row):
    wide = jnp.concatenate([row, jnp.zeros((1, 128 - row.shape[1]), f32)], axis=1)
    return jnp.broadcast_to(wide, (128, 128)).T


def front_kernel(
    tok, ng, wq_h, qg, wu_h, wl_h, lg, wr_h, qhg, khg, fine, coarse,
    normed, block, q_out,
    whole, wq, wu, wl, wr, wsem, s_r, r_r, s_l, r_l, s_fr, r_fr, s_fl, r_fl,
):
    sp = lax.axis_index("sp")
    me = lax.axis_index("tp")
    right, left = (me + 1) % 4, (me + 3) % 4
    loads = [
        pltpu.make_async_copy(src, dst, wsem.at[i])
        for i, (src, dst) in enumerate(((wl_h, wl), (wr_h, wr), (wq_h, wq), (wu_h, wu)))
    ]
    for load in loads:
        load.start()
    barrier = pltpu.get_barrier_semaphore()
    for peer in (left, right):
        pl.semaphore_signal(barrier, inc=1, device_id=(sp, peer), device_id_type=MESH)
    pl.semaphore_wait(barrier, 2)

    def rows_of(c, off=0, n=CHUNK):
        return pl.ds(pl.multiple_of(c * CHUNK + off, 16), n)

    def own(c, to, send, recv):
        return pltpu.make_async_remote_copy(
            src_ref=tok.at[rows_of(c)], dst_ref=whole.at[me, rows_of(c)],
            send_sem=send.at[c], recv_sem=recv.at[c], device_id=(sp, to), device_id_type=MESH,
        )

    def relay(c, owner, off, to, send, recv):
        part = whole.at[owner, rows_of(c, off, CHUNK // 2)]
        return pltpu.make_async_remote_copy(
            src_ref=part, dst_ref=part,
            send_sem=send.at[c], recv_sem=recv.at[c], device_id=(sp, to), device_id_type=MESH,
        )

    def rightward(c):
        return own(c, right, s_r, r_r)

    def leftward(c):
        return own(c, left, s_l, r_l)

    def relay_right(c):
        return relay(c, left, 0, right, s_fr, r_fr)

    def relay_left(c):
        return relay(c, right, CHUNK // 2, left, s_fl, r_fl)

    for c in range(2):
        rightward(c).start()
        leftward(c).start()
    whole[me] = tok[...]
    rightward(0).wait_recv()
    relay_right(0).start()
    leftward(0).wait_recv()
    relay_left(0).start()
    rightward(2).start()
    leftward(2).start()

    pick = lax.broadcasted_iota(jnp.int32, (16, 128), 1) == sp
    cc = jnp.sum(jnp.where(pick, coarse[0], 0.0), axis=1, keepdims=True)
    cs = jnp.sum(jnp.where(pick, coarse[1], 0.0), axis=1, keepdims=True)
    q_gain = column(qhg[...])
    k_gain = column(khg[...])
    for load in loads:
        load.wait()

    def step(c, carry):
        @pl.when(c < 2)
        def _():
            rightward(c + 1).wait_recv()
            relay_right(c + 1).start()
            leftward(c + 1).wait_recv()
            relay_left(c + 1).start()

        relay_right(c).wait_recv()
        relay_left(c).wait_recv()
        rows = rows_of(c)
        lanes = pl.ds(pl.multiple_of(c * CHUNK, 128), CHUNK)
        squares = jnp.zeros((CHUNK, 1), f32)
        for k in range(4):
            v = whole[k, rows].astype(f32)
            squares = squares + jnp.sum(v * v, axis=1, keepdims=True)
        scale = lax.rsqrt(squares * (1.0 / 2048) + eps)
        for k in range(4):
            v = whole[k, rows].astype(f32)
            normed[rows, k * 512 : (k + 1) * 512] = (
                v * scale * ng[:, k * 512 : (k + 1) * 512]
            ).astype(bf)
        here = normed[rows, :]
        lat = jnp.dot(here, wl[...], preferred_element_type=f32).astype(bf).astype(f32)
        lat = lat * lax.rsqrt(jnp.mean(lat * lat, axis=1, keepdims=True) + eps) * lg[...]
        block[0:LATENT, lanes] = lat.T.astype(bf)
        fc, fs = fine[0, :, lanes], fine[1, :, lanes]
        cosine = cc * fc - cs * fs
        sine = cs * fc + cc * fs

        def rotated(first, second):
            return first * cosine - second * sine, first * sine + second * cosine

        rot = jnp.dot(here, wr[...], preferred_element_type=f32).astype(bf).astype(f32)
        rot = jnp.concatenate([rot, jnp.zeros((CHUNK, 96), f32)], axis=1).T[0:ROPE]
        total = jnp.sum(rot * rot, axis=0, keepdims=True)
        high = total.astype(bf).astype(f32)
        low = total - high
        rot = rot * k_gain[NOPE:HEAD]
        first, second = rotated(rot[0:16], rot[16:32])
        line = lax.broadcasted_iota(jnp.int32, (16, CHUNK), 0)
        tail = jnp.where(line == 0, high, jnp.where(line == 1, low, 0.0))
        block[256:272, lanes] = first.astype(bf)
        block[272:288, lanes] = second.astype(bf)
        block[288:304, lanes] = tail.astype(bf)

        lat = jnp.dot(here, wq[...], preferred_element_type=f32).astype(bf).astype(f32)
        lat = lat * lax.rsqrt(jnp.mean(lat * lat, axis=1, keepdims=True) + eps) * qg[...]
        raw = jnp.dot(lat.astype(bf), wu[...], preferred_element_type=f32)
        raw = raw.astype(bf).astype(f32).T
        for h in range(HEADS_HERE):
            v = raw[h * HEAD : (h + 1) * HEAD]
            r = lax.rsqrt(jnp.mean(v * v, axis=0, keepdims=True) + eps)
            v = v * (r * (HEAD ** (-0.5) * LOG2E)) * q_gain[0:HEAD]
            first, second = rotated(v[64:80], v[80:96])
            v = jnp.concatenate(
                [v[0:NOPE] * k_gain[0:NOPE], first, second, jnp.zeros((32, CHUNK), f32)], axis=0
            )
            q_out[h, rows, :] = v.T.astype(bf)
        return carry

    lax.fori_loop(0, 3, step, 0)
    for c in range(3):
        for copy in (rightward(c), leftward(c), relay_right(c), relay_left(c)):
            copy.wait_send()


def front(tokens, norm_gain, wq, qg, wu, wl, lg, wr, qhg, khg):
    fine, coarse = rope_tables()
    vmem = pl.BlockSpec(memory_space=pltpu.VMEM)
    hbm = pl.BlockSpec(memory_space=pl.ANY)
    sems = pltpu.SemaphoreType.DMA((3,))
    return pl.pallas_call(
        front_kernel,
        out_shape=(
            jax.ShapeDtypeStruct((ROWS, 2048), bf),
            jax.ShapeDtypeStruct((KEY_ROWS, ROWS), bf),
            jax.ShapeDtypeStruct((HEADS_HERE, ROWS, 128), bf),
        ),
        in_specs=[vmem, vmem, hbm, vmem, hbm, hbm, vmem, hbm, vmem, vmem, vmem, vmem],
        out_specs=(vmem, vmem, vmem),
        scratch_shapes=[
            pltpu.VMEM((4, ROWS, 512), bf),
            pltpu.VMEM((2048, 512), bf),
            pltpu.VMEM((512, 384), bf),
            pltpu.VMEM((2048, 256), bf),
            pltpu.VMEM((2048, 32), bf),
            pltpu.SemaphoreType.DMA((4,)),
        ]
        + [sems] * 8,
        compiler_params=pltpu.CompilerParams(
            collective_id=0, has_side_effects=True, vmem_limit_bytes=40 * 2**20
        ),
        name="front",
    )(
        tokens, norm_gain.reshape(1, -1), wq, qg.reshape(1, -1), wu, wl, lg.reshape(1, -1), wr,
        qhg.reshape(1, -1), khg.reshape(1, -1), fine, coarse,
    )


ORDER = (
    (0, 0),
    (3, 0), (1, 0), (0, 3), (0, 1),
    (2, 0), (0, 2),
    (3, 3), (3, 1), (1, 3), (1, 1),
    (3, 2), (1, 2), (2, 3), (2, 1),
    (2, 2),
)
EVENTS = (1, 3, 6, 9, 11)
HALVES = ((0, 160), (160, 144))
PARTS = (((0, 80), (80, 80)), ((160, 80), (240, 64)))
STEPS = (1, 3)


def attend_kernel(
    q, block, w_up, out, g, acc, kt, vt, wt,
    s_own, r_own, s_1f, r_1f, s_1h, r_1h, s_2f, r_2f, s_2h, r_2h, s_d, r_d,
):
    sp = lax.axis_index("sp")
    tp = lax.axis_index("tp")
    core, y, z = sp % 2, (sp // 2) % 4, sp // 8
    partner = sp + 1 - 2 * core
    lanes = pl.ds(pl.multiple_of(core * ROWS, 128), ROWS)

    def slot(dy, dz):
        return ((z + dz) % 4) * 4 + (y + dy) % 4

    def device(dy, dz):
        return (slot(dy, dz) * 2 + core, tp)

    def offsets(half, along, across):
        return (along, across) if half == 0 else (across, along)

    def region(off, rows):
        return g.at[slot(*off), pl.ds(rows[0], rows[1]), lanes]

    def copy(src, dst, to, send, recv):
        return pltpu.make_async_remote_copy(
            src_ref=src, dst_ref=dst, send_sem=send, recv_sem=recv,
            device_id=to, device_id_type=MESH,
        )

    def mine(rows):
        return block.at[pl.ds(rows[0], rows[1]), :]

    def first_full(half, d):
        rows = HALVES[half]
        return copy(
            mine(rows), region((0, 0), rows), device(*offsets(half, STEPS[d], 0)),
            s_1f.at[half, d], r_1f.at[half, d],
        )

    def first_part(half, d):
        part = region(offsets(half, STEPS[1 - d], 0), PARTS[half][d])
        return copy(
            part, part, device(*offsets(half, STEPS[d], 0)),
            s_1h.at[half, d], r_1h.at[half, d],
        )

    def second_full(half, along, d):
        rows = HALVES[half]
        part = region(offsets(half, along, 0), rows)
        return copy(
            mine(rows) if along == 0 else part, part, device(*offsets(half, 0, STEPS[d])),
            s_2f.at[half, along, d], r_2f.at[half, along, d],
        )

    def second_part(half, along, d):
        part = region(offsets(half, along, STEPS[1 - d]), PARTS[half][d])
        return copy(
            part, part, device(*offsets(half, 0, STEPS[d])),
            s_2h.at[half, along, d], r_2h.at[half, along, d],
        )

    def across_chip(half, off):
        part = region(off, HALVES[half])
        at = off[0] * 4 + off[1]
        return copy(part, part, (partner, tp), s_d.at[half, at], r_d.at[half, at])

    def arrived_across(half, off):
        rows = HALVES[half]
        at = off[0] * 4 + off[1]
        there = g.at[
            slot(*off), pl.ds(rows[0], rows[1]),
            pl.ds(pl.multiple_of((1 - core) * ROWS, 128), ROWS),
        ]
        return copy(there, there, (partner, tp), s_d.at[half, at], r_d.at[half, at])

    own_across = copy(
        block, g.at[slot(0, 0), :, lanes], (partner, tp), s_own.at[0], r_own.at[0]
    )

    barrier = pltpu.get_barrier_semaphore()
    for off in ((1, 0), (3, 0), (0, 1), (0, 3)):
        pl.semaphore_signal(barrier, inc=1, device_id=device(*off), device_id_type=MESH)
    pl.semaphore_signal(barrier, inc=1, device_id=(partner, tp), device_id_type=MESH)
    pl.semaphore_wait(barrier, 5)

    own_across.start()
    for half in range(2):
        for d in range(2):
            first_full(half, d).start()
    for half in range(2):
        for d in range(2):
            second_full(half, 0, d).start()

    acc[...] = jnp.zeros_like(acc)
    g[slot(0, 0), :, lanes] = block[...]
    wt[...] = w_up[...].astype(f32).T.astype(bf)
    for h in range(HEADS_HERE):
        kt[h, HEAD:128] = jnp.zeros((32, 2 * ROWS), bf)
        vt[h, VALUE_DIM:128] = jnp.where(
            lax.broadcasted_iota(jnp.int32, (64, 2 * ROWS), 0) == 0, 1.0, 0.0
        ).astype(bf)
    own_across.wait_recv()

    def neighbours():
        for half in range(2):
            for d in range(2):
                first_full(half, d).wait_recv()
                first_part(half, d).start()
        for half in range(2):
            for d in range(2):
                second_full(half, 0, d).wait_recv()
                second_part(half, 0, d).start()
        for half in range(2):
            for d in range(2):
                across_chip(half, offsets(half, STEPS[1 - d], 0)).start()
                across_chip(half, offsets(half, 0, STEPS[1 - d])).start()
        for half in range(2):
            for d in range(2):
                for e in range(2):
                    second_full(half, STEPS[1 - d], e).start()

    def opposite():
        for half in range(2):
            for d in range(2):
                first_part(half, d).wait_recv()
            for e in range(2):
                second_full(half, 2, e).start()
            across_chip(half, offsets(half, 2, 0)).start()
            for d in range(2):
                second_part(half, 0, d).wait_recv()
            across_chip(half, offsets(half, 0, 2)).start()

    def diagonal():
        for half in range(2):
            for along in STEPS:
                for d in range(2):
                    second_full(half, along, d).wait_recv()
                    second_part(half, along, d).start()
                    across_chip(half, offsets(half, along, STEPS[1 - d])).start()

    def far():
        for half in range(2):
            for d in range(2):
                second_full(half, 2, d).wait_recv()
                second_part(half, 2, d).start()
                across_chip(half, offsets(half, 2, STEPS[1 - d])).start()
            for along in STEPS:
                for d in range(2):
                    second_part(half, along, d).wait_recv()
                across_chip(half, offsets(half, along, 2)).start()

    def farthest():
        for half in range(2):
            for d in range(2):
                second_part(half, 2, d).wait_recv()
            across_chip(half, (2, 2)).start()

    def chosen(t, values):
        return sum(jnp.where(t == k, v, 0) for k, v in enumerate(values) if v)

    def step(t, carry):
        for at, event in zip(EVENTS, (neighbours, opposite, diagonal, far, farthest)):
            pl.when(t == at)(event)
        dy = chosen(t, [o[0] for o in ORDER])
        dz = chosen(t, [o[1] for o in ORDER])

        @pl.when(t > 0)
        def _():
            for half in range(2):
                arrived_across(half, (dy, dz)).wait_recv()

        at = slot(dy, dz)
        lat = g[at, 0:LATENT, :]
        rot = g[at, LATENT : LATENT + ROPE, :].astype(f32)
        squares = g[at, LATENT + ROPE : KEY_ROWS, :].astype(f32)
        squares = squares[0:1] + squares[1:2]
        for h in range(HEADS_HERE):
            kv = jnp.dot(wt[h * 128 : (h + 1) * 128, :], lat, preferred_element_type=f32)
            k = kv[0:NOPE]
            r = lax.rsqrt((jnp.sum(k * k, axis=0, keepdims=True) + squares) * (1.0 / HEAD) + eps)
            kt[h, 0:NOPE] = (k * r).astype(bf)
            kt[h, NOPE:HEAD] = (rot * r).astype(bf)
            vt[h, 0:VALUE_DIM] = kv[NOPE:128].astype(bf)
        for h in range(HEADS_HERE):
            scores = jnp.dot(q[h], kt[h], preferred_element_type=f32)
            weights = jnp.exp2(scores).astype(bf)
            acc[h] += lax.dot_general(
                weights, vt[h], (((1,), (1,)), ((), ())), preferred_element_type=f32
            )
        return carry

    lax.fori_loop(0, 16, step, 0)
    for h in range(HEADS_HERE):
        a = acc[h]
        out[:, h * VALUE_DIM : (h + 1) * VALUE_DIM] = (
            a[:, 0:VALUE_DIM] / a[:, VALUE_DIM : VALUE_DIM + 1]
        ).astype(bf)

    own_across.wait_send()
    for half in range(2):
        for d in range(2):
            first_full(half, d).wait_send()
            first_part(half, d).wait_send()
            for along in range(4):
                second_full(half, along, d).wait_send()
                second_part(half, along, d).wait_send()
        for off in ORDER[1:]:
            across_chip(half, off).wait_send()


def attend(q, block, w_up):
    vmem = pl.BlockSpec(memory_space=pltpu.VMEM)
    dma = pltpu.SemaphoreType.DMA
    sems = []
    for shape in ((1,), (2, 2), (2, 2), (2, 4, 2), (2, 4, 2), (2, 16)):
        sems += [dma(shape), dma(shape)]
    return pl.pallas_call(
        attend_kernel,
        out_shape=jax.ShapeDtypeStruct((ROWS, HEADS_HERE * VALUE_DIM), bf),
        in_specs=[vmem, vmem, vmem],
        out_specs=vmem,
        scratch_shapes=[
            pltpu.VMEM((16, KEY_ROWS, 2 * ROWS), bf),
            pltpu.VMEM((HEADS_HERE, ROWS, 128), f32),
            pltpu.VMEM((HEADS_HERE, 128, 2 * ROWS), bf),
            pltpu.VMEM((HEADS_HERE, 128, 2 * ROWS), bf),
            pltpu.VMEM((HEADS_HERE * 128, LATENT), bf),
        ]
        + sems,
        compiler_params=pltpu.CompilerParams(
            collective_id=1, has_side_effects=True, vmem_limit_bytes=40 * 2**20
        ),
        name="attend",
    )(q, block, w_up)


def extended(cells, width):
    count = lax.axis_size("sp")
    ends = count - 1
    head = cells[:width]
    tail = cells[-width:]
    return jnp.concatenate(
        [
            lax.ppermute(tail, "sp", [(i, (i + 1) % count) for i in range(ends)]),
            cells,
            lax.ppermute(head, "sp", [((i + 1) % count, i) for i in range(ends)]),
        ],
        axis=0,
    )


def gathered_copies(value, axis, dim):
    copies = jnp.broadcast_to(value, (lax.axis_size(axis), *value.shape))
    parts = lax.all_to_all(copies, axis, split_axis=0, concat_axis=0, tiled=True)
    lengths = list(value.shape)
    lengths[dim] *= parts.shape[0]
    return jnp.moveaxis(parts, 0, dim).reshape(lengths)


def body(
    tokens, norm_gain, w_query_down, query_gain, w_query_up, w_latent_down, latent_gain,
    w_rotary_key, w_latent_up, query_head_gain, key_head_gain, w_pool_in, w_pool_mix, pool_scale,
    w_attn_out, w_pool_out, w_gate_attn, w_gate_pool,
):
    rows = tokens.shape[0]
    length = rows * lax.axis_size("sp")
    positions = lax.axis_index("sp") * rows + jnp.arange(rows, dtype=jnp.int32)
    normed, block, query = front(
        tokens, norm_gain, w_query_down, query_gain, w_query_up, w_latent_down, latent_gain,
        w_rotary_key, query_head_gain, key_head_gain,
    )
    attn_rows = attend(query, block, w_latent_up)
    pool_input = jnp.dot(normed, w_pool_in, preferred_element_type=f32).astype(bf)
    reach = 8
    window = jnp.power(2, lax.axis_index("tp") + 1)
    padded = extended(pool_input, reach)
    offs = jnp.arange(rows + 2 * reach)[None, :] - reach - jnp.arange(rows)[:, None]
    band = ((offs >= -(window // 2)) & (offs < window // 2)).astype(bf)
    pooled = jnp.dot(band, padded, preferred_element_type=f32)
    low = jnp.clip(positions[:, None] - window // 2, 0, length)
    high = jnp.clip(positions[:, None] + window // 2, 0, length)
    count = (high - low).astype(f32)
    pool_mixed = (pooled / count - pool_input.astype(f32)).astype(bf)
    grouped = jnp.dot(pool_mixed, w_pool_mix[0], preferred_element_type=f32)
    pool_rows = (grouped * pool_scale).astype(bf)
    gate_attn = jax.nn.sigmoid(jnp.dot(normed, w_gate_attn, preferred_element_type=f32))
    gate_pool = jax.nn.sigmoid(jnp.dot(normed, w_gate_pool, preferred_element_type=f32))
    attn_tokens = lax.all_to_all(attn_rows, "tp", split_axis=0, concat_axis=1, tiled=True)
    pool_tokens = lax.all_to_all(pool_rows, "tp", split_axis=0, concat_axis=1, tiled=True)
    both = gathered_copies(jnp.concatenate([w_attn_out, w_pool_out], axis=1), "tp", 0)
    width = w_attn_out.shape[1]
    attn_here = jnp.dot(attn_tokens, both[:, :width], preferred_element_type=f32)
    pool_here = jnp.dot(pool_tokens, both[:, width:], preferred_element_type=f32)
    attn_branch = lax.all_to_all(attn_here.astype(bf), "tp", split_axis=1, concat_axis=0, tiled=True)
    pool_branch = lax.all_to_all(pool_here.astype(bf), "tp", split_axis=1, concat_axis=0, tiled=True)
    return (gate_attn * attn_branch.astype(f32) + gate_pool * pool_branch.astype(f32)).astype(bf)


def solution(mesh):
    placed = (
        P("sp", "tp"), P(), P(), P(), P(None, "tp"), P(), P(), P(), P(None, "tp"), P(), P(),
        P(None, "tp"), P("tp", None, None), P("tp"), P("tp", None), P("tp", None),
        P(None, "tp"), P(None, "tp"),
    )
    return jax.shard_map(body, mesh=mesh, in_specs=placed, out_specs=P("sp", "tp"), check_vma=False)
```

```python
import numpy as np
import jax
import jax.numpy as jnp
from jax import lax
from jax.experimental import pallas as pl
from jax.experimental.pallas import tpu as pltpu
from jax.sharding import PartitionSpec as P

NOPE = 64
ROPE = 32
HEAD = NOPE + ROPE
VALUE_DIM = 64
ROWS = 384
HEADS_HERE = 4
LATENT = 256
KEY_ROWS = 304
CHUNK = 128
CHUNKS = 3
MESH = pl.DeviceIdType.MESH

eps = 1e-06
theta = 10000.0
LOG2E = 1.4426950408889634
bf = jnp.bfloat16
f32 = jnp.float32


def rope_tables():
    half = ROPE // 2
    freqs = theta ** (-np.arange(half, dtype=np.float64) / half)
    fine = np.arange(ROWS)[None, :] * freqs[:, None]
    coarse = (np.arange(128) * ROWS)[None, :] * freqs[:, None]
    fine = np.stack([np.cos(fine), np.sin(fine)]).astype(np.float32)
    coarse = np.stack([np.cos(coarse), np.sin(coarse)]).astype(np.float32)
    return fine, coarse


def column(row):
    wide = jnp.concatenate([row, jnp.zeros((1, 128 - row.shape[1]), f32)], axis=1)
    return jnp.broadcast_to(wide, (128, 128)).T


ORDER = (
    (0, 0),
    (3, 0), (1, 0), (0, 3), (0, 1),
    (2, 0), (0, 2),
    (3, 3), (3, 1), (1, 3), (1, 1),
    (3, 2), (1, 2), (2, 3), (2, 1),
    (2, 2),
)
HALVES = ((0, 160), (160, 144))
PARTS = (((0, 80), (80, 80)), ((160, 80), (240, 64)))
STEPS = (1, 3)


def mixer_kernel(
    tok, ng_h, wq_h, qg_h, wu_h, wl_h, lg_h, wr_h, wup_h, qhg_h, khg_h, wpi_h, mix_h, ps_h,
    wao_h, wpo_h, wga_h, wgp_h, fine_h, coarse_h,
    out,
    whole, ng, wq, qg, wu, wl, lg, wr, w_up, qhg, khg, wpi, mix, ps, wg, fine, coarse,
    normed, block, q, padded, g, acc, kt, vt, wt, gates, w_out, stage, prow, arow,
    load_sem, tok_sem, wown_sem, xt, xa, xp, xw, halo, s_across, r_across,
    s_1f, r_1f, s_1h, r_1h, s_2o, r_2o, s_2f, r_2f, s_2h, r_2h, s_d, r_d,
):
    sp = lax.axis_index("sp")
    tp = lax.axis_index("tp")
    core, y, z = sp % 2, (sp // 2) % 4, sp // 8
    partner = sp + 1 - 2 * core
    right, left, opposite_x = (tp + 1) % 4, (tp + 3) % 4, (tp + 2) % 4

    def copy(src, dst, to, send, recv):
        return pltpu.make_async_remote_copy(
            src_ref=src, dst_ref=dst, send_sem=send, recv_sem=recv,
            device_id=to, device_id_type=MESH,
        )

    def slot(dy, dz):
        return ((z + dz) % 4) * 4 + (y + dy) % 4

    def device(dy, dz):
        return (slot(dy, dz) * 2 + core, tp)

    def offsets(half, along, across):
        return (along, across) if half == 0 else (across, along)

    def lanes(c=None, whose=core):
        if c is None:
            return pl.ds(pl.multiple_of(whose * ROWS, 128), ROWS)
        return pl.ds(pl.multiple_of(whose * ROWS + c * CHUNK, 128), CHUNK)

    def chunk(c):
        return pl.ds(pl.multiple_of(c * CHUNK, 128), CHUNK)

    def region(off, rows, c=None):
        return g.at[slot(*off), pl.ds(rows[0], rows[1]), lanes(c)]

    def own_first(half, d, c):
        rows = HALVES[half]
        return copy(
            block.at[pl.ds(rows[0], rows[1]), chunk(c)], region((0, 0), rows, c),
            device(*offsets(half, STEPS[d], 0)), s_1f.at[half, d, c], r_1f.at[half, d, c],
        )

    def own_second(half, d, c):
        rows = HALVES[half]
        return copy(
            block.at[pl.ds(rows[0], rows[1]), chunk(c)], region((0, 0), rows, c),
            device(*offsets(half, 0, STEPS[d])), s_2o.at[half, d, c], r_2o.at[half, d, c],
        )

    def own_across(c):
        return copy(
            block.at[:, chunk(c)], g.at[slot(0, 0), :, lanes(c)], (partner, tp),
            s_across.at[c], r_across.at[c],
        )

    def first_part(half, d):
        part = region(offsets(half, STEPS[1 - d], 0), PARTS[half][d])
        return copy(
            part, part, device(*offsets(half, STEPS[d], 0)),
            s_1h.at[half, d], r_1h.at[half, d],
        )

    def second_full(half, along, d):
        part = region(offsets(half, along, 0), HALVES[half])
        return copy(
            part, part, device(*offsets(half, 0, STEPS[d])),
            s_2f.at[half, along, d], r_2f.at[half, along, d],
        )

    def second_part(half, along, d):
        part = region(offsets(half, along, STEPS[1 - d]), PARTS[half][d])
        return copy(
            part, part, device(*offsets(half, 0, STEPS[d])),
            s_2h.at[half, along, d], r_2h.at[half, along, d],
        )

    def across_chip(half, off):
        part = region(off, HALVES[half])
        at = off[0] * 4 + off[1]
        return copy(part, part, (partner, tp), s_d.at[half, at], r_d.at[half, at])

    def arrived_across(half, off):
        rows = HALVES[half]
        at = off[0] * 4 + off[1]
        there = g.at[slot(*off), pl.ds(rows[0], rows[1]), lanes(whose=1 - core)]
        return copy(there, there, (partner, tp), s_d.at[half, at], r_d.at[half, at])

    def along_x(buf, first, n, sem, kind, i):
        to = right if kind % 2 == 0 else left
        if kind < 2:
            part = buf.at[tp, pl.ds(first, n)]
        elif kind == 2:
            part = buf.at[left, pl.ds(first, n // 2)]
        else:
            part = buf.at[right, pl.ds(pl.multiple_of(first + n // 2, 16), n // 2)]
        return copy(part, part, (sp, to), sem.at[0, kind, i], sem.at[1, kind, i])

    def token_copy(kind, c):
        return along_x(whole, pl.multiple_of(c * CHUNK, CHUNK), CHUNK, xt, kind, c)

    def attn_copy(kind, c):
        return along_x(arow, c * CHUNK, CHUNK, xa, kind, c)

    def pool_copy(kind):
        return along_x(prow, 0, ROWS, xp, kind, 0)

    def columns(j):
        return pl.ds(pl.multiple_of(j * 512, 512), 512)

    w_src = (wao_h, wpo_h)

    def weight_copy(kind, w):
        to = right if kind % 2 == 0 else left
        if kind < 2:
            src, dst = w_src[w].at[:, columns(to)], w_out.at[w, tp]
        elif kind < 4:
            src = w_src[w].at[pl.ds(128 * (kind - 2), 128), columns(opposite_x)]
            dst = stage.at[w, kind - 2]
        else:
            src = stage.at[w, kind - 4]
            dst = w_out.at[w, left if kind == 4 else right, pl.ds(128 * (kind - 4), 128)]
        return copy(src, dst, (sp, to), xw.at[0, kind, w], xw.at[1, kind, w])

    def halo_copy(kind):
        if kind == 0:
            src, dst, to = padded.at[384:400], padded.at[0:16], (sp + 1) % 32
        else:
            src, dst, to = padded.at[16:32], padded.at[400:416], (sp + 31) % 32
        return copy(src, dst, (to, tp), halo.at[0, kind], halo.at[1, kind])

    own_tokens = pltpu.make_async_copy(tok, whole.at[tp], tok_sem.at[0])
    own_tokens.start()
    pairs = (
        (ng_h, ng), (fine_h, fine), (coarse_h, coarse), (qhg_h, qhg), (khg_h, khg), (lg_h, lg),
        (qg_h, qg), (wl_h, wl), (wr_h, wr), (wq_h, wq), (wu_h, wu), (wpi_h, wpi),
        (mix_h, mix), (ps_h, ps), (wup_h, w_up), (wga_h, wg.at[0]), (wgp_h, wg.at[1]),
    )
    loads = [pltpu.make_async_copy(s, d, load_sem.at[i]) for i, (s, d) in enumerate(pairs)]
    for load in loads:
        load.start()
    own_weights = [
        pltpu.make_async_copy(w_src[w].at[:, columns(tp)], w_out.at[w, tp], wown_sem.at[w])
        for w in range(2)
    ]

    barrier = pltpu.get_barrier_semaphore()
    far_neighbour = jnp.where(core == 0, (sp + 31) % 32, (sp + 1) % 32)
    peers = [(sp, right), (sp, left), (partner, tp), (far_neighbour, tp)]
    peers += [device(*off) for off in ((1, 0), (3, 0), (0, 1), (0, 3))]
    for peer in peers:
        pl.semaphore_signal(barrier, inc=1, device_id=peer, device_id_type=MESH)
    own_tokens.wait()
    pl.semaphore_wait(barrier, len(peers))

    for c in range(2):
        for kind in range(2):
            token_copy(kind, c).start()
    for load in loads[:7]:
        load.wait()
    pick = lax.broadcasted_iota(jnp.int32, (16, 128), 1) == sp
    cc = jnp.sum(jnp.where(pick, coarse[0], 0.0), axis=1, keepdims=True)
    cs = jnp.sum(jnp.where(pick, coarse[1], 0.0), axis=1, keepdims=True)
    q_gain = column(qhg[...])
    k_gain = column(khg[...])
    for kind in range(2):
        token_copy(kind, 0).wait_recv()
        token_copy(kind + 2, 0).start()
    for kind in range(2):
        token_copy(kind, 2).start()
    for load in loads[7:]:
        load.wait()

    def front_step(c, carry):
        @pl.when(c < CHUNKS - 1)
        def _():
            for kind in range(2):
                token_copy(kind, c + 1).wait_recv()
                token_copy(kind + 2, c + 1).start()

        for kind in range(2):
            token_copy(kind + 2, c).wait_recv()
        rows = chunk(c)
        squares = jnp.zeros((CHUNK, 1), f32)
        for k in range(4):
            v = whole[k, rows].astype(f32)
            squares = squares + jnp.sum(v * v, axis=1, keepdims=True)
        scale = lax.rsqrt(squares * (1.0 / 2048) + eps)
        for k in range(4):
            v = whole[k, rows].astype(f32)
            normed[rows, k * 512 : (k + 1) * 512] = (
                v * scale * ng[:, k * 512 : (k + 1) * 512]
            ).astype(bf)
        here = normed[rows, :]
        lat = jnp.dot(here, wl[...], preferred_element_type=f32).astype(bf).astype(f32)
        lat = lat * lax.rsqrt(jnp.mean(lat * lat, axis=1, keepdims=True) + eps) * lg[...]
        lat = lat.T.astype(bf)
        fc, fs = fine[0, :, rows], fine[1, :, rows]
        cosine = cc * fc - cs * fs
        sine = cs * fc + cc * fs

        def rotated(first, second):
            return first * cosine - second * sine, first * sine + second * cosine

        rot = lax.dot_general(
            wr[...], here, (((1,), (1,)), ((), ())), preferred_element_type=f32
        ).astype(bf).astype(f32)
        total = jnp.sum(rot * rot, axis=0, keepdims=True)
        high = total.astype(bf).astype(f32)
        low = total - high
        rot = rot * k_gain[NOPE:HEAD]
        first, second = rotated(rot[0:16], rot[16:32])
        line = lax.broadcasted_iota(jnp.int32, (16, CHUNK), 0)
        tail = jnp.where(line == 0, high, jnp.where(line == 1, low, 0.0))
        made = jnp.concatenate(
            [lat, first.astype(bf), second.astype(bf), tail.astype(bf)], axis=0
        )
        block[:, rows] = made
        g[slot(0, 0), :, lanes(c)] = made

        lat = jnp.dot(here, wq[...], preferred_element_type=f32).astype(bf).astype(f32)
        lat = lat * lax.rsqrt(jnp.mean(lat * lat, axis=1, keepdims=True) + eps) * qg[...]
        raw = jnp.dot(lat.astype(bf), wu[...], preferred_element_type=f32)
        own_across(c).start()
        for half in range(2):
            for d in range(2):
                own_first(half, d, c).start()
        for half in range(2):
            for d in range(2):
                own_second(half, d, c).start()
        raw = raw.astype(bf).astype(f32).T
        for h in range(HEADS_HERE):
            v = raw[h * HEAD : (h + 1) * HEAD]
            r = lax.rsqrt(jnp.mean(v * v, axis=0, keepdims=True) + eps)
            v = v * (r * (HEAD ** (-0.5) * LOG2E)) * q_gain[0:HEAD]
            first, second = rotated(v[64:80], v[80:96])
            v = jnp.concatenate(
                [v[0:NOPE] * k_gain[0:NOPE], first, second, jnp.zeros((32, CHUNK), f32)], axis=0
            )
            q[h, rows, :] = v.T.astype(bf)
        padded[pl.ds(pl.multiple_of(c * CHUNK + 16, 16), CHUNK), :] = jnp.dot(
            here, wpi[...], preferred_element_type=f32
        ).astype(bf)
        return carry

    lax.fori_loop(0, CHUNKS, front_step, 0)
    for w in range(2):
        for kind in (2, 3):
            weight_copy(kind, w).start()
    for kind in (0, 1):
        weight_copy(kind, 0).start()
    for own in own_weights:
        own.start()

    acc[...] = jnp.zeros_like(acc)
    wt[...] = w_up[...].astype(f32).T.astype(bf)
    for h in range(HEADS_HERE):
        kt[h, HEAD:128] = jnp.zeros((32, 2 * ROWS), bf)
        vt[h, VALUE_DIM:128] = jnp.where(
            lax.broadcasted_iota(jnp.int32, (64, 2 * ROWS), 0) == 0, 1.0, 0.0
        ).astype(bf)
    for kind in range(2):
        halo_copy(kind).start()
    for c in range(CHUNKS):
        own_across(c).wait_recv()

    def gates_and_pool():
        for k in range(2):
            for n in range(2):
                cols = slice(n * 256, (n + 1) * 256)
                gates[k, :, cols] = jax.nn.sigmoid(
                    jnp.dot(normed[...], wg[k, :, cols], preferred_element_type=f32)
                )
        for kind in range(2):
            halo_copy(kind).wait_recv()
        reach = jnp.where(tp == 0, 1, jnp.where(tp == 1, 2, jnp.where(tp == 2, 4, 8)))
        source = lax.broadcasted_iota(jnp.int32, (ROWS, ROWS + 32), 1) - 16
        offs = source - lax.broadcasted_iota(jnp.int32, (ROWS, ROWS + 32), 0)
        source = source + sp * ROWS
        length = 32 * ROWS
        inside = (offs >= -reach) & (offs < reach) & (source >= 0) & (source < length)
        band = jnp.where(inside, 1.0, 0.0).astype(bf)
        pooled = jnp.dot(band, padded[...], preferred_element_type=f32)
        at = sp * ROWS + lax.broadcasted_iota(jnp.int32, (ROWS, 1), 0)
        count = (jnp.minimum(at + reach, length) - jnp.maximum(at - reach, 0)).astype(f32)
        mixed = (pooled / count - padded[16:400].astype(f32)).astype(bf)
        grouped = jnp.dot(mixed, mix[0], preferred_element_type=f32)
        prow[tp] = (grouped * ps[...]).astype(bf)

    def neighbours():
        for half in range(2):
            for d in range(2):
                for c in range(CHUNKS):
                    own_first(half, d, c).wait_recv()
                first_part(half, d).start()
        for half in range(2):
            for d in range(2):
                for c in range(CHUNKS):
                    own_second(half, d, c).wait_recv()
                second_part(half, 0, d).start()
        for half in range(2):
            for d in range(2):
                across_chip(half, offsets(half, STEPS[1 - d], 0)).start()
                across_chip(half, offsets(half, 0, STEPS[1 - d])).start()
        for half in range(2):
            for d in range(2):
                for e in range(2):
                    second_full(half, STEPS[1 - d], e).start()

    def send_pool():
        for kind in range(2):
            pool_copy(kind).start()

    def opposite():
        for half in range(2):
            for d in range(2):
                first_part(half, d).wait_recv()
            for e in range(2):
                second_full(half, 2, e).start()
            across_chip(half, offsets(half, 2, 0)).start()
            for d in range(2):
                second_part(half, 0, d).wait_recv()
            across_chip(half, offsets(half, 0, 2)).start()

    def pass_weights():
        for w in range(2):
            for kind in (2, 3):
                weight_copy(kind, w).wait_recv()
                weight_copy(kind + 2, w).start()
        for kind in (0, 1):
            weight_copy(kind, 1).start()

    def diagonal():
        for half in range(2):
            for along in STEPS:
                for d in range(2):
                    second_full(half, along, d).wait_recv()
                    second_part(half, along, d).start()
                    across_chip(half, offsets(half, along, STEPS[1 - d])).start()

    def pass_pool():
        for kind in range(2):
            pool_copy(kind).wait_recv()
            pool_copy(kind + 2).start()

    def far():
        for half in range(2):
            for d in range(2):
                second_full(half, 2, d).wait_recv()
                second_part(half, 2, d).start()
                across_chip(half, offsets(half, 2, STEPS[1 - d])).start()
            for along in STEPS:
                for d in range(2):
                    second_part(half, along, d).wait_recv()
                across_chip(half, offsets(half, along, 2)).start()

    def farthest():
        for half in range(2):
            for d in range(2):
                second_part(half, 2, d).wait_recv()
            across_chip(half, (2, 2)).start()

    events = (
        (1, gates_and_pool), (1, neighbours), (1, send_pool), (3, opposite), (4, pass_weights),
        (6, diagonal), (8, pass_pool), (9, far), (11, farthest),
    )

    def chosen(t, values):
        return sum(jnp.where(t == k, v, 0) for k, v in enumerate(values) if v)

    def step(t, carry):
        for at, event in events:
            pl.when(t == at)(event)
        dy = chosen(t, [o[0] for o in ORDER])
        dz = chosen(t, [o[1] for o in ORDER])

        @pl.when(t > 0)
        def _():
            for half in range(2):
                arrived_across(half, (dy, dz)).wait_recv()

        at = slot(dy, dz)
        lat = g[at, 0:LATENT, :]
        rot = g[at, LATENT : LATENT + ROPE, :].astype(f32)
        squares = g[at, LATENT + ROPE : KEY_ROWS, :].astype(f32)
        squares = squares[0:1] + squares[1:2]
        for h in range(HEADS_HERE):
            kv = jnp.dot(wt[h * 128 : (h + 1) * 128, :], lat, preferred_element_type=f32)
            k = kv[0:NOPE]
            r = lax.rsqrt((jnp.sum(k * k, axis=0, keepdims=True) + squares) * (1.0 / HEAD) + eps)
            kt[h, 0:NOPE] = (k * r).astype(bf)
            kt[h, NOPE:HEAD] = (rot * r).astype(bf)
            vt[h, 0:VALUE_DIM] = kv[NOPE:128].astype(bf)
        for h in range(HEADS_HERE):
            scores = jnp.dot(q[h], kt[h], preferred_element_type=f32)
            weights = jnp.exp2(scores).astype(bf)
            acc[h] += lax.dot_general(
                weights, vt[h], (((1,), (1,)), ((), ())), preferred_element_type=f32
            )
        return carry

    lax.fori_loop(0, 16, step, 0)

    for c in range(CHUNKS):
        rows = slice(c * CHUNK, (c + 1) * CHUNK)
        for h in range(HEADS_HERE):
            a = acc[h, rows]
            arow[tp, rows, h * VALUE_DIM : (h + 1) * VALUE_DIM] = (
                a[:, 0:VALUE_DIM] / a[:, VALUE_DIM : VALUE_DIM + 1]
            ).astype(bf)
        if c > 0:
            for kind in range(2):
                attn_copy(kind, c - 1).start()
    for own in own_weights:
        own.wait()
    for w in range(2):
        for kind in (0, 1, 4, 5):
            weight_copy(kind, w).wait_recv()
    for kind in range(2):
        attn_copy(kind, CHUNKS - 1).start()
        pool_copy(kind + 2).wait_recv()

    def projected(buf, rows, w):
        return sum(
            jnp.dot(buf[k, rows], w_out[w, k], preferred_element_type=f32) for k in range(4)
        )

    everything = slice(0, ROWS)
    gates[1] = gates[1] * projected(prow, everything, 1)
    for c in range(CHUNKS):
        for kind in range(2):
            attn_copy(kind, c).wait_recv()
            attn_copy(kind + 2, c).start()
    for c in range(CHUNKS):
        rows = slice(c * CHUNK, (c + 1) * CHUNK)
        for kind in range(2):
            attn_copy(kind + 2, c).wait_recv()
        out[rows, :] = (gates[0, rows] * projected(arow, rows, 0) + gates[1, rows]).astype(bf)

    for c in range(CHUNKS):
        for kind in range(4):
            token_copy(kind, c).wait_send()
            attn_copy(kind, c).wait_send()
        own_across(c).wait_send()
        for half in range(2):
            for d in range(2):
                own_first(half, d, c).wait_send()
                own_second(half, d, c).wait_send()
    for kind in range(4):
        pool_copy(kind).wait_send()
    for w in range(2):
        for kind in range(6):
            weight_copy(kind, w).wait_send()
    for half in range(2):
        halo_copy(half).wait_send()
        for d in range(2):
            first_part(half, d).wait_send()
            for along in range(4):
                if along:
                    second_full(half, along, d).wait_send()
                second_part(half, along, d).wait_send()
        for off in ORDER[1:]:
            across_chip(half, off).wait_send()


def body(
    tokens, norm_gain, w_query_down, query_gain, w_query_up, w_latent_down, latent_gain,
    w_rotary_key, w_latent_up, query_head_gain, key_head_gain, w_pool_in, w_pool_mix, pool_scale,
    w_attn_out, w_pool_out, w_gate_attn, w_gate_pool,
):
    fine, coarse = rope_tables()

    def row(v):
        return v.reshape(1, -1)

    args = (
        tokens, row(norm_gain), w_query_down, row(query_gain), w_query_up, w_latent_down,
        row(latent_gain), w_rotary_key.T, w_latent_up, row(query_head_gain), row(key_head_gain),
        w_pool_in, w_pool_mix, row(pool_scale), w_attn_out, w_pool_out, w_gate_attn, w_gate_pool,
        fine, coarse,
    )
    dma = pltpu.SemaphoreType.DMA
    sems = [dma((17,)), dma((1,)), dma((2,)), dma((2, 4, 3)), dma((2, 4, 3)), dma((2, 4, 1))]
    sems += [dma((2, 6, 2)), dma((2, 2)), dma((3,)), dma((3,))]
    for shape in ((2, 2, 3), (2, 2), (2, 2, 3), (2, 4, 2), (2, 4, 2), (2, 16)):
        sems += [dma(shape), dma(shape)]
    return pl.pallas_call(
        mixer_kernel,
        out_shape=jax.ShapeDtypeStruct((ROWS, 512), bf),
        in_specs=[pl.BlockSpec(memory_space=pl.ANY)] * len(args),
        out_specs=pl.BlockSpec(memory_space=pltpu.VMEM),
        scratch_shapes=[
            pltpu.VMEM((4, ROWS, 512), bf),
            pltpu.VMEM((1, 2048), f32),
            pltpu.VMEM((2048, 512), bf),
            pltpu.VMEM((1, 512), f32),
            pltpu.VMEM((512, 384), bf),
            pltpu.VMEM((2048, 256), bf),
            pltpu.VMEM((1, 256), f32),
            pltpu.VMEM((32, 2048), bf),
            pltpu.VMEM((256, 512), bf),
            pltpu.VMEM((1, 96), f32),
            pltpu.VMEM((1, 96), f32),
            pltpu.VMEM((2048, 256), bf),
            pltpu.VMEM((1, 256, 256), bf),
            pltpu.VMEM((1, 256), f32),
            pltpu.VMEM((2, 2048, 512), bf),
            pltpu.VMEM((2, 16, ROWS), f32),
            pltpu.VMEM((2, 16, 128), f32),
            pltpu.VMEM((ROWS, 2048), bf),
            pltpu.VMEM((KEY_ROWS, ROWS), bf),
            pltpu.VMEM((HEADS_HERE, ROWS, 128), bf),
            pltpu.VMEM((ROWS + 32, 256), bf),
            pltpu.VMEM((16, KEY_ROWS, 2 * ROWS), bf),
            pltpu.VMEM((HEADS_HERE, ROWS, 128), f32),
            pltpu.VMEM((HEADS_HERE, 128, 2 * ROWS), bf),
            pltpu.VMEM((HEADS_HERE, 128, 2 * ROWS), bf),
            pltpu.VMEM((HEADS_HERE * 128, LATENT), bf),
            pltpu.VMEM((2, ROWS, 512), f32),
            pltpu.VMEM((2, 4, 256, 512), bf),
            pltpu.VMEM((2, 2, 128, 512), bf),
            pltpu.VMEM((4, ROWS, 256), bf),
            pltpu.VMEM((4, ROWS, 256), bf),
        ]
        + sems,
        compiler_params=pltpu.CompilerParams(
            collective_id=0, has_side_effects=True, vmem_limit_bytes=63 * 2**20
        ),
        name="mixer",
    )(*args)


def solution(mesh):
    placed = (
        P("sp", "tp"), P(), P(), P(), P(None, "tp"), P(), P(), P(), P(None, "tp"), P(), P(),
        P(None, "tp"), P("tp", None, None), P("tp"), P("tp", None), P("tp", None),
        P(None, "tp"), P(None, "tp"),
    )
    return jax.shard_map(body, mesh=mesh, in_specs=placed, out_specs=P("sp", "tp"), check_vma=False)
```

```python
import numpy as np
import jax
import jax.numpy as jnp
from jax import lax
from jax.experimental import pallas as pl
from jax.experimental.pallas import tpu as pltpu
from jax.sharding import PartitionSpec as P

NOPE = 64
ROPE = 32
HEAD = NOPE + ROPE
VALUE_DIM = 64
ROWS = 384
HEADS_HERE = 4
LATENT = 256
KEY_ROWS = 304
CHUNK = 128
CHUNKS = 3
MESH = pl.DeviceIdType.MESH

eps = 1e-06
theta = 10000.0
LOG2E = 1.4426950408889634
bf = jnp.bfloat16
f32 = jnp.float32


def rope_tables():
    half = ROPE // 2
    freqs = theta ** (-np.arange(half, dtype=np.float64) / half)
    fine = np.arange(ROWS)[None, :] * freqs[:, None]
    coarse = (np.arange(128) * ROWS)[None, :] * freqs[:, None]
    fine = np.stack([np.cos(fine), np.sin(fine)]).astype(np.float32)
    coarse = np.stack([np.cos(coarse), np.sin(coarse)]).astype(np.float32)
    return fine, coarse


def column(row):
    wide = jnp.concatenate([row, jnp.zeros((1, 128 - row.shape[1]), f32)], axis=1)
    return jnp.broadcast_to(wide, (128, 128)).T


ORDER = (
    (0, 0),
    (3, 0), (1, 0), (0, 3), (0, 1),
    (2, 0), (0, 2),
    (3, 3), (3, 1), (1, 3), (1, 1),
    (3, 2), (1, 2), (2, 3), (2, 1),
    (2, 2),
)
EVENTS = (4, 5, 5, 7, 9, 9, 12)
FULL = 11
EARLY_GATES = 1
FILL_GATES = 2
CODES = tuple(
    int(np.uint32(sum(off[i] << (2 * k) for k, off in enumerate(ORDER))).astype(np.int32))
    for i in range(2)
)
HALVES = ((0, 160), (160, 144))
PARTS = (((0, 80), (80, 80)), ((160, 80), (240, 64)))
STEPS = (1, 3)


def mixer_kernel(
    tok, ng_h, wq_h, qg_h, wu_h, wl_h, lg_h, wr_h, wup_h, qhg_h, khg_h, wpi_h, mix_h, ps_h,
    wao_h, wpo_h, wga_h, wgp_h, fine_h, coarse_h,
    out,
    whole, ng, wq, qg, wu, wl, lg, wr, w_up, qhg, khg, wpi, mix, ps, wg, fine, coarse,
    normed, block, q, padded, g, acc, kt_a, vt_a, kt_b, vt_b, wt, gates, part, w_out, stage,
    prow, arow,
    load_sem, tok_sem, wown_sem, xt, xa, xp, xw, halo, s_across, r_across,
    s_1f, r_1f, s_1h, r_1h, s_2o, r_2o, s_2f, r_2f, s_2h, r_2h, s_d, r_d,
):
    sp = lax.axis_index("sp")
    tp = lax.axis_index("tp")
    core, y, z = sp % 2, (sp // 2) % 4, sp // 8
    partner = sp + 1 - 2 * core
    right, left, opposite_x = (tp + 1) % 4, (tp + 3) % 4, (tp + 2) % 4

    def copy(src, dst, to, send, recv):
        return pltpu.make_async_remote_copy(
            src_ref=src, dst_ref=dst, send_sem=send, recv_sem=recv,
            device_id=to, device_id_type=MESH,
        )

    def slot(dy, dz):
        return ((z + dz) % 4) * 4 + (y + dy) % 4

    def device(dy, dz):
        return (slot(dy, dz) * 2 + core, tp)

    def offsets(half, along, across):
        return (along, across) if half == 0 else (across, along)

    def lanes(c=None, whose=core):
        if c is None:
            return pl.ds(pl.multiple_of(whose * ROWS, 128), ROWS)
        return pl.ds(pl.multiple_of(whose * ROWS + c * CHUNK, 128), CHUNK)

    def chunk(c):
        return pl.ds(pl.multiple_of(c * CHUNK, 128), CHUNK)

    def region(off, rows, c=None):
        return g.at[slot(*off), pl.ds(rows[0], rows[1]), lanes(c)]

    def own_first(half, d, c):
        rows = HALVES[half]
        return copy(
            block.at[pl.ds(rows[0], rows[1]), chunk(c)], region((0, 0), rows, c),
            device(*offsets(half, STEPS[d], 0)), s_1f.at[half, d, c], r_1f.at[half, d, c],
        )

    def own_second(half, d, c):
        rows = HALVES[half]
        return copy(
            block.at[pl.ds(rows[0], rows[1]), chunk(c)], region((0, 0), rows, c),
            device(*offsets(half, 0, STEPS[d])), s_2o.at[half, d, c], r_2o.at[half, d, c],
        )

    def own_across(c):
        return copy(
            block.at[:, chunk(c)], g.at[slot(0, 0), :, lanes(c)], (partner, tp),
            s_across.at[c], r_across.at[c],
        )

    def first_part(half, d, c=None):
        part = region(offsets(half, STEPS[1 - d], 0), PARTS[half][d], c)
        return copy(
            part, part, device(*offsets(half, STEPS[d], 0)),
            s_1h.at[half, d], r_1h.at[half, d],
        )

    def second_full(half, along, d, c=None):
        part = region(offsets(half, along, 0), HALVES[half], c)
        return copy(
            part, part, device(*offsets(half, 0, STEPS[d])),
            s_2f.at[half, along, d], r_2f.at[half, along, d],
        )

    def second_part(half, along, d, c=None):
        part = region(offsets(half, along, STEPS[1 - d]), PARTS[half][d], c)
        return copy(
            part, part, device(*offsets(half, 0, STEPS[d])),
            s_2h.at[half, along, d], r_2h.at[half, along, d],
        )

    def across_chip(half, off, c=None):
        part = region(off, HALVES[half], c)
        at = off[0] * 4 + off[1]
        return copy(part, part, (partner, tp), s_d.at[half, at], r_d.at[half, at])

    def arrived_across(half, off):
        rows = HALVES[half]
        at = off[0] * 4 + off[1]
        there = g.at[slot(*off), pl.ds(rows[0], rows[1]), lanes(whose=1 - core)]
        return copy(there, there, (partner, tp), s_d.at[half, at], r_d.at[half, at])

    def along_x(buf, first, n, sem, kind, i):
        to = right if kind % 2 == 0 else left
        if kind < 2:
            part = buf.at[tp, pl.ds(first, n)]
        elif kind == 2:
            part = buf.at[left, pl.ds(first, n // 2)]
        else:
            part = buf.at[right, pl.ds(pl.multiple_of(first + n // 2, 16), n // 2)]
        return copy(part, part, (sp, to), sem.at[0, kind, i], sem.at[1, kind, i])

    def token_copy(kind, c):
        return along_x(whole, pl.multiple_of(c * CHUNK, CHUNK), CHUNK, xt, kind, c)

    def attn_copy(kind, pair, c):
        return along_x(arow.at[pair], c * CHUNK, CHUNK, xa, kind, pair * CHUNKS + c)

    def pool_copy(kind):
        return along_x(prow, 0, ROWS, xp, kind, 0)

    def columns(j):
        return pl.ds(pl.multiple_of(j * 512, 512), 512)

    w_src = (wao_h, wpo_h)

    def weight_copy(kind, w=None):
        to = right if kind % 2 == 0 else left
        if kind < 2:
            src = w_src[w or 0].at[:, columns(to)]
            dst = w_out.at[core, tp]
        elif kind < 4:
            src = w_src[w or 0].at[pl.ds(128 * (kind - 2), 128), columns(opposite_x)]
            dst = stage.at[kind - 2]
        elif kind < 6:
            src = stage.at[kind - 4]
            dst = w_out.at[core, left if kind == 4 else right, pl.ds(128 * (kind - 4), 128)]
        else:
            src = dst = w_out.at[core, (left, right, opposite_x)[kind - 6]]
        peer = (sp, to) if kind < 6 else (partner, tp)
        return copy(src, dst, peer, xw.at[0, kind], xw.at[1, kind])

    def send_weights(kinds):
        for w in range(2):

            @pl.when(core == w)
            def _():
                for kind in kinds:
                    weight_copy(kind, w).start()

    def halo_copy(kind):
        if kind == 0:
            src, dst, to = padded.at[384:400], padded.at[0:16], (sp + 1) % 32
        else:
            src, dst, to = padded.at[16:32], padded.at[400:416], (sp + 31) % 32
        return copy(src, dst, (to, tp), halo.at[0, kind], halo.at[1, kind])

    own_tokens = pltpu.make_async_copy(tok, whole.at[tp], tok_sem.at[0])
    own_tokens.start()
    pairs = (
        (ng_h, ng), (fine_h, fine), (coarse_h, coarse), (qhg_h, qhg), (khg_h, khg), (lg_h, lg),
        (qg_h, qg), (wl_h, wl), (wr_h, wr), (wq_h, wq), (wu_h, wu), (wpi_h, wpi),
        (mix_h, mix), (ps_h, ps), (wup_h, w_up), (wga_h, wg.at[0]), (wgp_h, wg.at[1]),
    )
    loads = [pltpu.make_async_copy(s, d, load_sem.at[i]) for i, (s, d) in enumerate(pairs)]
    own_weights = [
        pltpu.make_async_copy(w_src[w].at[:, columns(tp)], w_out.at[w, tp], wown_sem.at[w])
        for w in range(2)
    ]

    barrier = pltpu.get_barrier_semaphore()
    far_neighbour = jnp.where(core == 0, (sp + 31) % 32, (sp + 1) % 32)
    peers = [(sp, right), (sp, left), (partner, tp), (far_neighbour, tp)]
    peers += [device(*off) for off in ((1, 0), (3, 0), (0, 1), (0, 3))]
    for peer in peers:
        pl.semaphore_signal(barrier, inc=1, device_id=peer, device_id_type=MESH)
    own_tokens.wait()
    for load in loads:
        load.start()
    pl.semaphore_wait(barrier, len(peers))

    for c in range(2):
        for kind in range(2):
            token_copy(kind, c).start()
    for load in loads[:7]:
        load.wait()
    pick = lax.broadcasted_iota(jnp.int32, (16, 128), 1) == sp
    cc = jnp.sum(jnp.where(pick, coarse[0], 0.0), axis=1, keepdims=True)
    cs = jnp.sum(jnp.where(pick, coarse[1], 0.0), axis=1, keepdims=True)
    q_gain = column(qhg[...])
    k_gain = column(khg[...])
    for kind in range(2):
        token_copy(kind, 0).wait_recv()
        token_copy(kind + 2, 0).start()
    for kind in range(2):
        token_copy(kind, 2).start()
    for load in loads[7:]:
        load.wait()

    def neighbours(c):
        for half in range(2):
            for d in range(2):
                own_first(half, d, c).wait_recv()
                first_part(half, d, c).start()
        for half in range(2):
            for d in range(2):
                own_second(half, d, c).wait_recv()
                second_part(half, 0, d, c).start()
        for half in range(2):
            for d in range(2):
                across_chip(half, offsets(half, STEPS[1 - d], 0), c).start()
                across_chip(half, offsets(half, 0, STEPS[1 - d]), c).start()
        for half in range(2):
            for d in range(2):
                for e in range(2):
                    second_full(half, STEPS[1 - d], e, c).start()

    def gate_rows(c):
        rows = slice(c * CHUNK, (c + 1) * CHUNK)
        for k in range(2):
            gates[k, rows] = jax.nn.sigmoid(
                jnp.dot(normed[rows, :], wg[k], preferred_element_type=f32)
            )

    def front_step(c, carry):
        @pl.when(c < CHUNKS - 1)
        def _():
            for kind in range(2):
                token_copy(kind, c + 1).wait_recv()
                token_copy(kind + 2, c + 1).start()

        @pl.when(c == CHUNKS - 1)
        def _():
            for early in range(EARLY_GATES):
                gate_rows(early)

        for kind in range(2):
            token_copy(kind + 2, c).wait_recv()
        rows = chunk(c)
        squares = jnp.zeros((CHUNK, 1), f32)
        for k in range(4):
            v = whole[k, rows].astype(f32)
            squares = squares + jnp.sum(v * v, axis=1, keepdims=True)
        scale = lax.rsqrt(squares * (1.0 / 2048) + eps)
        for k in range(4):
            v = whole[k, rows].astype(f32)
            normed[rows, k * 512 : (k + 1) * 512] = (
                v * scale * ng[:, k * 512 : (k + 1) * 512]
            ).astype(bf)
        here = normed[rows, :]
        lat = jnp.dot(here, wl[...], preferred_element_type=f32).astype(bf).astype(f32)
        lat = lat * lax.rsqrt(jnp.mean(lat * lat, axis=1, keepdims=True) + eps) * lg[...]
        lat = lat.T.astype(bf)
        fc, fs = fine[0, :, rows], fine[1, :, rows]
        cosine = cc * fc - cs * fs
        sine = cs * fc + cc * fs

        def rotated(first, second):
            return first * cosine - second * sine, first * sine + second * cosine

        rot = lax.dot_general(
            wr[...], here, (((1,), (1,)), ((), ())), preferred_element_type=f32
        ).astype(bf).astype(f32)
        total = jnp.sum(rot * rot, axis=0, keepdims=True)
        high = total.astype(bf).astype(f32)
        low = total - high
        rot = rot * k_gain[NOPE:HEAD]
        first, second = rotated(rot[0:16], rot[16:32])
        line = lax.broadcasted_iota(jnp.int32, (16, CHUNK), 0)
        tail = jnp.where(line == 0, high, jnp.where(line == 1, low, 0.0))
        made = jnp.concatenate(
            [lat, first.astype(bf), second.astype(bf), tail.astype(bf)], axis=0
        )
        block[:, rows] = made
        g[slot(0, 0), :, lanes(c)] = made

        lat = jnp.dot(here, wq[...], preferred_element_type=f32).astype(bf).astype(f32)
        lat = lat * lax.rsqrt(jnp.mean(lat * lat, axis=1, keepdims=True) + eps) * qg[...]
        raw = jnp.dot(lat.astype(bf), wu[...], preferred_element_type=f32)
        own_across(c).start()
        for half in range(2):
            for d in range(2):
                own_first(half, d, c).start()
        for half in range(2):
            for d in range(2):
                own_second(half, d, c).start()
        raw = raw.astype(bf).astype(f32).T
        for h in range(HEADS_HERE):
            v = raw[h * HEAD : (h + 1) * HEAD]
            r = lax.rsqrt(jnp.mean(v * v, axis=0, keepdims=True) + eps)
            v = v * (r * (HEAD ** (-0.5) * LOG2E)) * q_gain[0:HEAD]
            first, second = rotated(v[64:80], v[80:96])
            v = jnp.concatenate(
                [v[0:NOPE] * k_gain[0:NOPE], first, second, jnp.zeros((32, CHUNK), f32)], axis=0
            )
            q[h, rows, :] = v.T.astype(bf)
        padded[pl.ds(pl.multiple_of(c * CHUNK + 16, 16), CHUNK), :] = jnp.dot(
            here, wpi[...], preferred_element_type=f32
        ).astype(bf)

        @pl.when(c == CHUNKS - 1)
        def _():
            neighbours(0)

        return carry

    lax.fori_loop(0, CHUNKS, front_step, 0)
    send_weights((2, 3, 0, 1))
    for own in own_weights:
        own.start()

    acc[...] = jnp.zeros_like(acc)
    for h in range(HEADS_HERE):
        wt[h] = w_up[:, h * 128 : (h + 1) * 128].astype(f32).T.astype(bf)
    for kt, vt in ((kt_a, vt_a), (kt_b, vt_b)):
        for h in range(HEADS_HERE):
            kt[h, HEAD:128] = jnp.zeros((32, 2 * ROWS), bf)
            vt[h, VALUE_DIM:128] = jnp.where(
                lax.broadcasted_iota(jnp.int32, (64, 2 * ROWS), 0) == 0, 1.0, 0.0
            ).astype(bf)
    for kind in range(2):
        halo_copy(kind).start()
    for c in range(CHUNKS):
        own_across(c).wait_recv()

    def pool():
        for kind in range(2):
            halo_copy(kind).wait_recv()
        reach = jnp.where(tp == 0, 1, jnp.where(tp == 1, 2, jnp.where(tp == 2, 4, 8)))
        source = lax.broadcasted_iota(jnp.int32, (ROWS, ROWS + 32), 1) - 16
        offs = source - lax.broadcasted_iota(jnp.int32, (ROWS, ROWS + 32), 0)
        source = source + sp * ROWS
        length = 32 * ROWS
        inside = (offs >= -reach) & (offs < reach) & (source >= 0) & (source < length)
        band = jnp.where(inside, 1.0, 0.0).astype(bf)
        pooled = jnp.dot(band, padded[...], preferred_element_type=f32)
        at = sp * ROWS + lax.broadcasted_iota(jnp.int32, (ROWS, 1), 0)
        count = (jnp.minimum(at + reach, length) - jnp.maximum(at - reach, 0)).astype(f32)
        mixed = (pooled / count - padded[16:400].astype(f32)).astype(bf)
        grouped = jnp.dot(mixed, mix[0], preferred_element_type=f32)
        prow[tp] = (grouped * ps[...]).astype(bf)

    def send_pool():
        for kind in range(2):
            pool_copy(kind).start()

    def opposite():
        for half in range(2):
            for d in range(2):
                first_part(half, d).wait_recv()
            for e in range(2):
                second_full(half, 2, e).start()
            across_chip(half, offsets(half, 2, 0)).start()
            for d in range(2):
                second_part(half, 0, d).wait_recv()
            across_chip(half, offsets(half, 0, 2)).start()

    def pass_weights():
        for kind in (2, 3):
            weight_copy(kind).wait_recv()
            weight_copy(kind + 2).start()

    def share_weights():
        for kind in (0, 1, 4, 5):
            weight_copy(kind).wait_recv()
        for kind in (6, 7, 8):
            weight_copy(kind).start()

    def diagonal():
        for half in range(2):
            for along in STEPS:
                for d in range(2):
                    second_full(half, along, d).wait_recv()
                    second_part(half, along, d).start()
                    across_chip(half, offsets(half, along, STEPS[1 - d])).start()

    def pass_pool():
        for kind in range(2):
            pool_copy(kind).wait_recv()
            pool_copy(kind + 2).start()

    def far():
        for half in range(2):
            for d in range(2):
                second_full(half, 2, d).wait_recv()
                second_part(half, 2, d).start()
                across_chip(half, offsets(half, 2, STEPS[1 - d])).start()
            for along in STEPS:
                for d in range(2):
                    second_part(half, along, d).wait_recv()
                across_chip(half, offsets(half, along, 2)).start()

    def farthest():
        for half in range(2):
            for d in range(2):
                second_part(half, 2, d).wait_recv()
            across_chip(half, (2, 2)).start()

    def finish(pair):
        for c in range(CHUNKS):
            rows = slice(c * CHUNK, (c + 1) * CHUNK)
            for i in range(2):
                a = acc[2 * pair + i, rows]
                arow[pair, tp, rows, i * VALUE_DIM : (i + 1) * VALUE_DIM] = (
                    a[:, 0:VALUE_DIM] / a[:, VALUE_DIM : VALUE_DIM + 1]
                ).astype(bf)

    def send_rows(pair, c):
        for kind in range(2):
            attn_copy(kind, pair, c).start()

    def first_rows():
        finish(0)
        for c in range(CHUNKS):
            send_rows(0, c)

    def pass_rows():
        for c in range(CHUNKS):
            for kind in range(2):
                attn_copy(kind, 0, c).wait_recv()
                attn_copy(kind + 2, 0, c).start()

    def slot_of(b):
        return slot(*((code >> (2 * b)) & 3 for code in CODES))

    def landed(b):
        dy, dz = ((code >> (2 * b)) & 3 for code in CODES)
        for half in range(2):
            arrived_across(half, (dy, dz)).wait_recv()

    def prepare(b, heads, kt, vt):
        at = slot_of(b)
        lat = g[at, 0:LATENT, :]
        rot = g[at, LATENT : LATENT + ROPE, :].astype(f32)
        squares = g[at, LATENT + ROPE : KEY_ROWS, :].astype(f32)
        squares = squares[0:1] + squares[1:2]
        for h in heads:
            kv = jnp.dot(wt[h], lat, preferred_element_type=f32)
            k = kv[0:NOPE]
            r = lax.rsqrt((jnp.sum(k * k, axis=0, keepdims=True) + squares) * (1.0 / HEAD) + eps)
            kt[h, 0:NOPE] = (k * r).astype(bf)
            kt[h, NOPE:HEAD] = (rot * r).astype(bf)
            vt[h, 0:VALUE_DIM] = kv[NOPE:128].astype(bf)

    def attend(heads, kt, vt):
        for h in heads:
            scores = jnp.dot(q[h], kt[h], preferred_element_type=f32)
            weights = jnp.exp2(scores).astype(bf)
            acc[h] += lax.dot_general(
                weights, vt[h], (((1,), (1,)), ((), ())), preferred_element_type=f32
            )

    every = range(HEADS_HERE)
    prepare(0, every, kt_a, vt_a)
    for c in range(EARLY_GATES, FILL_GATES):
        gate_rows(c)
    attend(every, kt_a, vt_a)
    neighbours(1)
    for c in range(FILL_GATES, CHUNKS):
        gate_rows(c)
    neighbours(2)
    pool()
    landed(1)
    send_pool()
    prepare(1, every, kt_a, vt_a)
    events = tuple(zip(EVENTS, (
        opposite, pass_weights, diagonal, pass_pool, share_weights, far, farthest,
    )))

    def pairs_of_blocks(first, heads, arriving):
        def step(n, carry):
            b = 2 * n + first
            for off, (k_now, v_now, k_next, v_next) in (
                (1, (kt_a, vt_a, kt_b, vt_b)), (2, (kt_b, vt_b, kt_a, vt_a))
            ):
                if arriving:
                    for at, event in events:
                        if at in range(first + off, first + 2 * steps + off, 2):
                            pl.when(b + off == at)(event)
                    landed(b + off)
                attend(heads, k_now, v_now)
                prepare(b + off, heads, k_next, v_next)
            return carry

        steps = ((FULL if first == 1 else 15) - first) // 2
        lax.fori_loop(0, steps, step, 0)

    pairs_of_blocks(1, every, True)
    pairs_of_blocks(FULL, (0, 1), True)
    attend((0, 1), kt_a, vt_a)
    first_rows()
    pairs_of_blocks(FULL, (2, 3), False)
    attend((2, 3), kt_a, vt_a)

    finish(1)
    for own in own_weights:
        own.wait()
    for kind in (6, 7, 8):
        there = w_out.at[1 - core, (left, right, opposite_x)[kind - 6]]
        copy(there, there, (partner, tp), xw.at[0, kind], xw.at[1, kind]).wait_recv()
    for c in range(CHUNKS):
        send_rows(1, c)
    pass_rows()
    for kind in range(2):
        pool_copy(kind + 2).wait_recv()
    gates[1] = gates[1] * sum(
        jnp.dot(prow[k], w_out[1, k], preferred_element_type=f32) for k in range(4)
    )
    for c in range(CHUNKS):
        for kind in range(2):
            attn_copy(kind, 1, c).wait_recv()
            attn_copy(kind + 2, 1, c).start()

    def projected(pair, rows):
        return sum(
            jnp.dot(
                arow[pair, k, rows], w_out[0, k, pair * 128 : (pair + 1) * 128],
                preferred_element_type=f32,
            )
            for k in range(4)
        )

    for c in range(CHUNKS):
        for kind in range(2):
            attn_copy(kind + 2, 0, c).wait_recv()
    part[...] = projected(0, slice(0, ROWS))
    for c in range(CHUNKS):
        rows = slice(c * CHUNK, (c + 1) * CHUNK)
        for kind in range(2):
            attn_copy(kind + 2, 1, c).wait_recv()
        out[rows, :] = (
            gates[0, rows] * (part[rows] + projected(1, rows)) + gates[1, rows]
        ).astype(bf)

    for c in range(CHUNKS):
        for kind in range(4):
            token_copy(kind, c).wait_send()
            for pair in range(2):
                attn_copy(kind, pair, c).wait_send()
        own_across(c).wait_send()
        for half in range(2):
            for d in range(2):
                own_first(half, d, c).wait_send()
                own_second(half, d, c).wait_send()
    for kind in range(4):
        pool_copy(kind).wait_send()
    for kind in range(9):
        weight_copy(kind).wait_send()
    for half in range(2):
        halo_copy(half).wait_send()
        for d in range(2):
            first_part(half, d).wait_send()
            for along in range(4):
                if along:
                    second_full(half, along, d).wait_send()
                second_part(half, along, d).wait_send()
        for off in ORDER[1:]:
            across_chip(half, off).wait_send()


def body(
    tokens, norm_gain, w_query_down, query_gain, w_query_up, w_latent_down, latent_gain,
    w_rotary_key, w_latent_up, query_head_gain, key_head_gain, w_pool_in, w_pool_mix, pool_scale,
    w_attn_out, w_pool_out, w_gate_attn, w_gate_pool,
):
    fine, coarse = rope_tables()

    def row(v):
        return v.reshape(1, -1)

    args = (
        tokens, row(norm_gain), w_query_down, row(query_gain), w_query_up, w_latent_down,
        row(latent_gain), w_rotary_key.T, w_latent_up, row(query_head_gain), row(key_head_gain),
        w_pool_in, w_pool_mix, row(pool_scale), w_attn_out, w_pool_out, w_gate_attn, w_gate_pool,
        fine, coarse,
    )
    dma = pltpu.SemaphoreType.DMA
    sems = [dma((17,)), dma((1,)), dma((2,)), dma((2, 4, 3)), dma((2, 4, 6)), dma((2, 4, 1))]
    sems += [dma((2, 9)), dma((2, 2)), dma((3,)), dma((3,))]
    for shape in ((2, 2, 3), (2, 2), (2, 2, 3), (2, 4, 2), (2, 4, 2), (2, 16)):
        sems += [dma(shape), dma(shape)]
    return pl.pallas_call(
        mixer_kernel,
        out_shape=pltpu.VMEM((ROWS, 512), bf),
        in_specs=[pl.BlockSpec(memory_space=pl.ANY)] * len(args),
        out_specs=pl.BlockSpec(memory_space=pltpu.VMEM),
        scratch_shapes=[
            pltpu.VMEM((4, ROWS, 512), bf),
            pltpu.VMEM((1, 2048), f32),
            pltpu.VMEM((2048, 512), bf),
            pltpu.VMEM((1, 512), f32),
            pltpu.VMEM((512, 384), bf),
            pltpu.VMEM((2048, 256), bf),
            pltpu.VMEM((1, 256), f32),
            pltpu.VMEM((32, 2048), bf),
            pltpu.VMEM((256, 512), bf),
            pltpu.VMEM((1, 96), f32),
            pltpu.VMEM((1, 96), f32),
            pltpu.VMEM((2048, 256), bf),
            pltpu.VMEM((1, 256, 256), bf),
            pltpu.VMEM((1, 256), f32),
            pltpu.VMEM((2, 2048, 512), bf),
            pltpu.VMEM((2, 16, ROWS), f32),
            pltpu.VMEM((2, 16, 128), f32),
            pltpu.VMEM((ROWS, 2048), bf),
            pltpu.VMEM((KEY_ROWS, ROWS), bf),
            pltpu.VMEM((HEADS_HERE, ROWS, 128), bf),
            pltpu.VMEM((ROWS + 32, 256), bf),
            pltpu.VMEM((16, KEY_ROWS, 2 * ROWS), bf),
            pltpu.VMEM((HEADS_HERE, ROWS, 128), f32),
            pltpu.VMEM((HEADS_HERE, 128, 2 * ROWS), bf),
            pltpu.VMEM((HEADS_HERE, 128, 2 * ROWS), bf),
            pltpu.VMEM((HEADS_HERE, 128, 2 * ROWS), bf),
            pltpu.VMEM((HEADS_HERE, 128, 2 * ROWS), bf),
            pltpu.VMEM((HEADS_HERE, 128, LATENT), bf),
            pltpu.VMEM((2, ROWS, 512), f32),
            pltpu.VMEM((ROWS, 512), f32),
            pltpu.VMEM((2, 4, 256, 512), bf),
            pltpu.VMEM((2, 128, 512), bf),
            pltpu.VMEM((4, ROWS, 256), bf),
            pltpu.VMEM((2, 4, ROWS, 128), bf),
        ]
        + sems,
        compiler_params=pltpu.CompilerParams(
            collective_id=0, has_side_effects=True, vmem_limit_bytes=60 * 2**20
        ),
        name="mixer",
    )(*args)


def solution(mesh):
    placed = (
        P("sp", "tp"), P(), P(), P(), P(None, "tp"), P(), P(), P(), P(None, "tp"), P(), P(),
        P(None, "tp"), P("tp", None, None), P("tp"), P("tp", None), P("tp", None),
        P(None, "tp"), P(None, "tp"),
    )
    return jax.shard_map(body, mesh=mesh, in_specs=placed, out_specs=P("sp", "tp"), check_vma=False)
```

```python
import numpy as np
import jax
import jax.numpy as jnp
from jax import lax
from jax.experimental import pallas as pl
from jax.experimental.pallas import tpu as pltpu
from jax.sharding import PartitionSpec as P

NOPE = 64
ROPE = 32
HEAD = NOPE + ROPE
VALUE_DIM = 64
ROWS = 384
HEADS_HERE = 4
LATENT = 256
KEY_ROWS = 304
CHUNK = 128
CHUNKS = 3
MESH = pl.DeviceIdType.MESH

eps = 1e-06
theta = 10000.0
LOG2E = 1.4426950408889634
bf = jnp.bfloat16
f32 = jnp.float32


def rope_tables():
    half = ROPE // 2
    freqs = theta ** (-np.arange(half, dtype=np.float64) / half)
    fine = np.arange(ROWS)[None, :] * freqs[:, None]
    coarse = (np.arange(128) * ROWS)[None, :] * freqs[:, None]
    fine = np.stack([np.cos(fine), np.sin(fine)]).astype(np.float32)
    coarse = np.stack([np.cos(coarse), np.sin(coarse)]).astype(np.float32)
    return fine, coarse


def column(row):
    wide = jnp.concatenate([row, jnp.zeros((1, 128 - row.shape[1]), f32)], axis=1)
    return jnp.broadcast_to(wide, (128, 128)).T


ORDER = (
    (0, 0),
    (3, 0), (1, 0), (0, 3), (0, 1),
    (2, 0), (0, 2),
    (3, 3), (3, 1), (1, 3), (1, 1),
    (3, 2), (1, 2), (2, 3), (2, 1),
    (2, 2),
)
EVENTS = (4, 5, 5, 7, 9, 9, 12)
FULL = 11
CODES = tuple(
    int(np.uint32(sum(off[i] << (2 * k) for k, off in enumerate(ORDER))).astype(np.int32))
    for i in range(2)
)
HALVES = ((0, 160), (160, 144))
PARTS = (((0, 80), (80, 80)), ((160, 80), (240, 64)))
STEPS = (1, 3)


def mixer_kernel(
    tok, ng_h, wq_h, qg_h, wu_h, wl_h, lg_h, wr_h, wup_h, qhg_h, khg_h, wpi_h, mix_h, ps_h,
    wao_h, wpo_h, wga_h, wgp_h, fine_h, coarse_h,
    out,
    whole, ng, wq, qg, wu, wl, lg, wr, w_up, qhg, khg, wpi, mix, ps, wg, fine, coarse,
    normed, block, q, padded, g, acc, kt_a, vt_a, kt_b, vt_b, wt, gates, part, w_out, stage,
    prow, arow,
    load_sem, tok_sem, wown_sem, xt, xa, xp, xw, halo, s_across, r_across,
    s_1f, r_1f, s_1h, r_1h, s_2o, r_2o, s_2f, r_2f, s_2h, r_2h, s_d, r_d,
):
    sp = lax.axis_index("sp")
    tp = lax.axis_index("tp")
    core, y, z = sp % 2, (sp // 2) % 4, sp // 8
    partner = sp + 1 - 2 * core
    right, left, opposite_x = (tp + 1) % 4, (tp + 3) % 4, (tp + 2) % 4

    def copy(src, dst, to, send, recv):
        return pltpu.make_async_remote_copy(
            src_ref=src, dst_ref=dst, send_sem=send, recv_sem=recv,
            device_id=to, device_id_type=MESH,
        )

    def slot(dy, dz):
        return ((z + dz) % 4) * 4 + (y + dy) % 4

    def device(dy, dz):
        return (slot(dy, dz) * 2 + core, tp)

    def offsets(half, along, across):
        return (along, across) if half == 0 else (across, along)

    def lanes(c=None, whose=core):
        if c is None:
            return pl.ds(pl.multiple_of(whose * ROWS, 128), ROWS)
        return pl.ds(pl.multiple_of(whose * ROWS + c * CHUNK, 128), CHUNK)

    def chunk(c):
        return pl.ds(pl.multiple_of(c * CHUNK, 128), CHUNK)

    def region(off, rows, c=None):
        return g.at[slot(*off), pl.ds(rows[0], rows[1]), lanes(c)]

    def own_first(half, d, c):
        rows = HALVES[half]
        return copy(
            block.at[pl.ds(rows[0], rows[1]), chunk(c)], region((0, 0), rows, c),
            device(*offsets(half, STEPS[d], 0)), s_1f.at[half, d, c], r_1f.at[half, d, c],
        )

    def own_second(half, d, c):
        rows = HALVES[half]
        return copy(
            block.at[pl.ds(rows[0], rows[1]), chunk(c)], region((0, 0), rows, c),
            device(*offsets(half, 0, STEPS[d])), s_2o.at[half, d, c], r_2o.at[half, d, c],
        )

    def own_across(c):
        return copy(
            block.at[:, chunk(c)], g.at[slot(0, 0), :, lanes(c)], (partner, tp),
            s_across.at[c], r_across.at[c],
        )

    def first_part(half, d, c=None):
        part = region(offsets(half, STEPS[1 - d], 0), PARTS[half][d], c)
        return copy(
            part, part, device(*offsets(half, STEPS[d], 0)),
            s_1h.at[half, d], r_1h.at[half, d],
        )

    def second_full(half, along, d, c=None):
        part = region(offsets(half, along, 0), HALVES[half], c)
        return copy(
            part, part, device(*offsets(half, 0, STEPS[d])),
            s_2f.at[half, along, d], r_2f.at[half, along, d],
        )

    def second_part(half, along, d, c=None):
        part = region(offsets(half, along, STEPS[1 - d]), PARTS[half][d], c)
        return copy(
            part, part, device(*offsets(half, 0, STEPS[d])),
            s_2h.at[half, along, d], r_2h.at[half, along, d],
        )

    def across_chip(half, off, c=None):
        part = region(off, HALVES[half], c)
        at = off[0] * 4 + off[1]
        return copy(part, part, (partner, tp), s_d.at[half, at], r_d.at[half, at])

    def arrived_across(half, off):
        rows = HALVES[half]
        at = off[0] * 4 + off[1]
        there = g.at[slot(*off), pl.ds(rows[0], rows[1]), lanes(whose=1 - core)]
        return copy(there, there, (partner, tp), s_d.at[half, at], r_d.at[half, at])

    def along_x(buf, first, n, sem, kind, i):
        to = right if kind % 2 == 0 else left
        if kind < 2:
            part = buf.at[tp, pl.ds(first, n)]
        elif kind == 2:
            part = buf.at[left, pl.ds(first, n // 2)]
        else:
            part = buf.at[right, pl.ds(pl.multiple_of(first + n // 2, 16), n // 2)]
        return copy(part, part, (sp, to), sem.at[0, kind, i], sem.at[1, kind, i])

    PIECES = ((0, 128), (128, 128), (256, 64), (320, 64))
    OF_CHUNK = ((0,), (1,), (2, 3))

    def token_copy(kind, p):
        return along_x(whole, *PIECES[p], xt, kind, p)

    def relay_tokens(c):
        for p in OF_CHUNK[c]:
            for kind in range(2):
                token_copy(kind, p).wait_recv()
                token_copy(kind + 2, p).start()

    def all_tokens(c):
        for p in OF_CHUNK[c]:
            for kind in range(2):
                token_copy(kind + 2, p).wait_recv()

    def attn_copy(kind, pair, c):
        return along_x(arow.at[pair], c * CHUNK, CHUNK, xa, kind, pair * CHUNKS + c)

    def pool_copy(kind):
        return along_x(prow, 0, ROWS, xp, kind, 0)

    def columns(j):
        return pl.ds(pl.multiple_of(j * 512, 512), 512)

    w_src = (wao_h, wpo_h)

    def weight_copy(kind, w=None):
        to = right if kind % 2 == 0 else left
        if kind < 2:
            src = w_src[w or 0].at[:, columns(to)]
            dst = w_out.at[core, tp]
        elif kind < 4:
            src = w_src[w or 0].at[pl.ds(128 * (kind - 2), 128), columns(opposite_x)]
            dst = stage.at[kind - 2]
        elif kind < 6:
            src = stage.at[kind - 4]
            dst = w_out.at[core, left if kind == 4 else right, pl.ds(128 * (kind - 4), 128)]
        else:
            src = dst = w_out.at[core, (left, right, opposite_x)[kind - 6]]
        peer = (sp, to) if kind < 6 else (partner, tp)
        return copy(src, dst, peer, xw.at[0, kind], xw.at[1, kind])

    def send_weights(kinds):
        for w in range(2):

            @pl.when(core == w)
            def _():
                for kind in kinds:
                    weight_copy(kind, w).start()

    def halo_copy(kind):
        if kind == 0:
            src, dst, to = padded.at[384:400], padded.at[0:16], (sp + 1) % 32
        else:
            src, dst, to = padded.at[16:32], padded.at[400:416], (sp + 31) % 32
        return copy(src, dst, (to, tp), halo.at[0, kind], halo.at[1, kind])

    own_tokens = [
        pltpu.make_async_copy(
            tok.at[pl.ds(c * CHUNK, CHUNK)], whole.at[tp, pl.ds(c * CHUNK, CHUNK)], tok_sem.at[c]
        )
        for c in range(CHUNKS)
    ]
    for own in own_tokens:
        own.start()
    pairs = (
        (ng_h, ng), (fine_h, fine), (coarse_h, coarse), (qhg_h, qhg), (khg_h, khg), (lg_h, lg),
        (qg_h, qg), (wl_h, wl), (wr_h, wr), (wq_h, wq), (wu_h, wu), (wpi_h, wpi),
        (mix_h, mix), (ps_h, ps), (wup_h, w_up), (wga_h, wg.at[0]), (wgp_h, wg.at[1]),
    )
    loads = [pltpu.make_async_copy(s, d, load_sem.at[i]) for i, (s, d) in enumerate(pairs)]
    own_weights = [
        pltpu.make_async_copy(w_src[w].at[:, columns(tp)], w_out.at[w, tp], wown_sem.at[w])
        for w in range(2)
    ]

    barrier = pltpu.get_barrier_semaphore()
    far_neighbour = jnp.where(core == 0, (sp + 31) % 32, (sp + 1) % 32)
    peers = [(sp, right), (sp, left), (partner, tp), (far_neighbour, tp)]
    peers += [device(*off) for off in ((1, 0), (3, 0), (0, 1), (0, 3))]
    for peer in peers:
        pl.semaphore_signal(barrier, inc=1, device_id=peer, device_id_type=MESH)
    own_tokens[0].wait()
    for load in loads:
        load.start()
    pl.semaphore_wait(barrier, len(peers))

    for c in range(2):
        for kind in range(2):
            token_copy(kind, c).start()
        own_tokens[c + 1].wait()
    for load in loads[:7]:
        load.wait()
    pick = lax.broadcasted_iota(jnp.int32, (16, 128), 1) == sp
    cc = jnp.sum(jnp.where(pick, coarse[0], 0.0), axis=1, keepdims=True)
    cs = jnp.sum(jnp.where(pick, coarse[1], 0.0), axis=1, keepdims=True)
    q_gain = column(qhg[...])
    k_gain = column(khg[...])
    relay_tokens(0)
    for p in OF_CHUNK[2]:
        for kind in range(2):
            token_copy(kind, p).start()
    for load in loads[7:]:
        load.wait()

    def neighbours(c):
        for half in range(2):
            for d in range(2):
                own_first(half, d, c).wait_recv()
                first_part(half, d, c).start()
        for half in range(2):
            for d in range(2):
                own_second(half, d, c).wait_recv()
                second_part(half, 0, d, c).start()
        for half in range(2):
            for d in range(2):
                across_chip(half, offsets(half, STEPS[1 - d], 0), c).start()
                across_chip(half, offsets(half, 0, STEPS[1 - d]), c).start()
        for half in range(2):
            for d in range(2):
                for e in range(2):
                    second_full(half, STEPS[1 - d], e, c).start()

    def gate_rows(rows):
        for k in range(2):
            gates[k, rows] = jax.nn.sigmoid(
                jnp.dot(normed[rows, :], wg[k], preferred_element_type=f32)
            )

    def front_step(c, carry):
        for at in range(CHUNKS - 1):
            pl.when(c == at)(lambda at=at: relay_tokens(at + 1))

        @pl.when(c > 0)
        def _():
            gate_rows(chunk(c - 1))

        for at in range(CHUNKS):
            pl.when(c == at)(lambda at=at: all_tokens(at))
        rows = chunk(c)
        squares = jnp.zeros((CHUNK, 1), f32)
        for k in range(4):
            v = whole[k, rows].astype(f32)
            squares = squares + jnp.sum(v * v, axis=1, keepdims=True)
        scale = lax.rsqrt(squares * (1.0 / 2048) + eps)
        for k in range(4):
            v = whole[k, rows].astype(f32)
            normed[rows, k * 512 : (k + 1) * 512] = (
                v * scale * ng[:, k * 512 : (k + 1) * 512]
            ).astype(bf)
        here = normed[rows, :]
        lat = jnp.dot(here, wl[...], preferred_element_type=f32).astype(bf).astype(f32)
        lat = lat * lax.rsqrt(jnp.mean(lat * lat, axis=1, keepdims=True) + eps) * lg[...]
        lat = lat.T.astype(bf)
        fc, fs = fine[0, :, rows], fine[1, :, rows]
        cosine = cc * fc - cs * fs
        sine = cs * fc + cc * fs

        def rotated(first, second):
            return first * cosine - second * sine, first * sine + second * cosine

        rot = lax.dot_general(
            wr[...], here, (((1,), (1,)), ((), ())), preferred_element_type=f32
        ).astype(bf).astype(f32)
        total = jnp.sum(rot * rot, axis=0, keepdims=True)
        high = total.astype(bf).astype(f32)
        low = total - high
        rot = rot * k_gain[NOPE:HEAD]
        first, second = rotated(rot[0:16], rot[16:32])
        line = lax.broadcasted_iota(jnp.int32, (16, CHUNK), 0)
        tail = jnp.where(line == 0, high, jnp.where(line == 1, low, 0.0))
        made = jnp.concatenate(
            [lat, first.astype(bf), second.astype(bf), tail.astype(bf)], axis=0
        )
        block[:, rows] = made
        g[slot(0, 0), :, lanes(c)] = made
        own_across(c).start()
        for half in range(2):
            for d in range(2):
                own_first(half, d, c).start()
        for half in range(2):
            for d in range(2):
                own_second(half, d, c).start()

        lat = jnp.dot(here, wq[...], preferred_element_type=f32).astype(bf).astype(f32)
        lat = lat * lax.rsqrt(jnp.mean(lat * lat, axis=1, keepdims=True) + eps) * qg[...]
        raw = jnp.dot(lat.astype(bf), wu[...], preferred_element_type=f32)
        raw = raw.astype(bf).astype(f32).T
        for h in range(HEADS_HERE):
            v = raw[h * HEAD : (h + 1) * HEAD]
            r = lax.rsqrt(jnp.mean(v * v, axis=0, keepdims=True) + eps)
            v = v * (r * (HEAD ** (-0.5) * LOG2E)) * q_gain[0:HEAD]
            first, second = rotated(v[64:80], v[80:96])
            v = jnp.concatenate(
                [v[0:NOPE] * k_gain[0:NOPE], first, second, jnp.zeros((32, CHUNK), f32)], axis=0
            )
            q[h, rows, :] = v.T.astype(bf)
        padded[pl.ds(pl.multiple_of(c * CHUNK + 16, 16), CHUNK), :] = jnp.dot(
            here, wpi[...], preferred_element_type=f32
        ).astype(bf)

        @pl.when(c == CHUNKS - 1)
        def _():
            neighbours(0)

        return carry

    lax.fori_loop(0, CHUNKS, front_step, 0)
    send_weights((2, 3, 0, 1))
    for own in own_weights:
        own.start()

    acc[...] = jnp.zeros_like(acc)
    for h in range(HEADS_HERE):
        wt[h] = w_up[:, h * 128 : (h + 1) * 128].astype(f32).T.astype(bf)
    for kt, vt in ((kt_a, vt_a), (kt_b, vt_b)):
        for h in range(HEADS_HERE):
            kt[h, HEAD:128] = jnp.zeros((32, 2 * ROWS), bf)
            vt[h, VALUE_DIM:128] = jnp.where(
                lax.broadcasted_iota(jnp.int32, (64, 2 * ROWS), 0) == 0, 1.0, 0.0
            ).astype(bf)
    for kind in range(2):
        halo_copy(kind).start()
    for c in range(CHUNKS):
        own_across(c).wait_recv()

    def pool():
        for kind in range(2):
            halo_copy(kind).wait_recv()
        reach = jnp.where(tp == 0, 1, jnp.where(tp == 1, 2, jnp.where(tp == 2, 4, 8)))
        source = lax.broadcasted_iota(jnp.int32, (ROWS, ROWS + 32), 1) - 16
        offs = source - lax.broadcasted_iota(jnp.int32, (ROWS, ROWS + 32), 0)
        source = source + sp * ROWS
        length = 32 * ROWS
        inside = (offs >= -reach) & (offs < reach) & (source >= 0) & (source < length)
        band = jnp.where(inside, 1.0, 0.0).astype(bf)
        pooled = jnp.dot(band, padded[...], preferred_element_type=f32)
        at = sp * ROWS + lax.broadcasted_iota(jnp.int32, (ROWS, 1), 0)
        count = (jnp.minimum(at + reach, length) - jnp.maximum(at - reach, 0)).astype(f32)
        mixed = (pooled / count - padded[16:400].astype(f32)).astype(bf)
        grouped = jnp.dot(mixed, mix[0], preferred_element_type=f32)
        prow[tp] = (grouped * ps[...]).astype(bf)

    def send_pool():
        for kind in range(2):
            pool_copy(kind).start()

    def opposite():
        for half in range(2):
            for d in range(2):
                first_part(half, d).wait_recv()
            for e in range(2):
                second_full(half, 2, e).start()
            across_chip(half, offsets(half, 2, 0)).start()
            for d in range(2):
                second_part(half, 0, d).wait_recv()
            across_chip(half, offsets(half, 0, 2)).start()

    def pass_weights():
        for kind in (2, 3):
            weight_copy(kind).wait_recv()
            weight_copy(kind + 2).start()

    def share_weights():
        for kind in (0, 1, 4, 5):
            weight_copy(kind).wait_recv()
        for kind in (6, 7, 8):
            weight_copy(kind).start()

    def diagonal():
        for half in range(2):
            for along in STEPS:
                for d in range(2):
                    second_full(half, along, d).wait_recv()
                    second_part(half, along, d).start()
                    across_chip(half, offsets(half, along, STEPS[1 - d])).start()

    def pass_pool():
        for kind in range(2):
            pool_copy(kind).wait_recv()
            pool_copy(kind + 2).start()

    def far():
        for half in range(2):
            for d in range(2):
                second_full(half, 2, d).wait_recv()
                second_part(half, 2, d).start()
                across_chip(half, offsets(half, 2, STEPS[1 - d])).start()
            for along in STEPS:
                for d in range(2):
                    second_part(half, along, d).wait_recv()
                across_chip(half, offsets(half, along, 2)).start()

    def farthest():
        for half in range(2):
            for d in range(2):
                second_part(half, 2, d).wait_recv()
            across_chip(half, (2, 2)).start()

    def finish(pair):
        for c in range(CHUNKS):
            rows = slice(c * CHUNK, (c + 1) * CHUNK)
            for i in range(2):
                a = acc[2 * pair + i, rows]
                arow[pair, tp, rows, i * VALUE_DIM : (i + 1) * VALUE_DIM] = (
                    a[:, 0:VALUE_DIM] / a[:, VALUE_DIM : VALUE_DIM + 1]
                ).astype(bf)

    def send_rows(pair, c):
        for kind in range(2):
            attn_copy(kind, pair, c).start()

    def first_rows():
        finish(0)
        for c in range(CHUNKS):
            send_rows(0, c)

    def pass_rows():
        for c in range(CHUNKS):
            for kind in range(2):
                attn_copy(kind, 0, c).wait_recv()
                attn_copy(kind + 2, 0, c).start()

    def slot_of(b):
        return slot(*((code >> (2 * b)) & 3 for code in CODES))

    def landed(b):
        dy, dz = ((code >> (2 * b)) & 3 for code in CODES)
        for half in range(2):
            arrived_across(half, (dy, dz)).wait_recv()

    def prepare(b, heads, kt, vt):
        at = slot_of(b)
        lat = g[at, 0:LATENT, :]
        rot = g[at, LATENT : LATENT + ROPE, :].astype(f32)
        squares = g[at, LATENT + ROPE : KEY_ROWS, :].astype(f32)
        squares = squares[0:1] + squares[1:2]
        for h in heads:
            kv = jnp.dot(wt[h], lat, preferred_element_type=f32)
            k = kv[0:NOPE]
            r = lax.rsqrt((jnp.sum(k * k, axis=0, keepdims=True) + squares) * (1.0 / HEAD) + eps)
            kt[h, 0:NOPE] = (k * r).astype(bf)
            kt[h, NOPE:HEAD] = (rot * r).astype(bf)
            vt[h, 0:VALUE_DIM] = kv[NOPE:128].astype(bf)

    def attend(heads, kt, vt):
        for h in heads:
            scores = jnp.dot(q[h], kt[h], preferred_element_type=f32)
            weights = jnp.exp2(scores).astype(bf)
            acc[h] += lax.dot_general(
                weights, vt[h], (((1,), (1,)), ((), ())), preferred_element_type=f32
            )

    every = range(HEADS_HERE)
    prepare(0, every, kt_a, vt_a)
    attend(every, kt_a, vt_a)
    neighbours(1)
    gate_rows(slice(ROWS - CHUNK, ROWS))
    neighbours(2)
    pool()
    landed(1)
    send_pool()
    prepare(1, every, kt_a, vt_a)
    events = tuple(zip(EVENTS, (
        opposite, pass_weights, diagonal, pass_pool, share_weights, far, farthest,
    )))

    def pairs_of_blocks(first, heads, arriving):
        def step(n, carry):
            b = 2 * n + first
            for off, (k_now, v_now, k_next, v_next) in (
                (1, (kt_a, vt_a, kt_b, vt_b)), (2, (kt_b, vt_b, kt_a, vt_a))
            ):
                if arriving:
                    for at, event in events:
                        if at in range(first + off, first + 2 * steps + off, 2):
                            pl.when(b + off == at)(event)
                    landed(b + off)
                attend(heads, k_now, v_now)
                prepare(b + off, heads, k_next, v_next)
            return carry

        steps = ((FULL if first == 1 else 15) - first) // 2
        lax.fori_loop(0, steps, step, 0)

    pairs_of_blocks(1, every, True)
    pairs_of_blocks(FULL, (0, 1), True)
    attend((0, 1), kt_a, vt_a)
    first_rows()
    pairs_of_blocks(FULL, (2, 3), False)
    attend((2, 3), kt_a, vt_a)

    finish(1)
    for own in own_weights:
        own.wait()
    for kind in (6, 7, 8):
        there = w_out.at[1 - core, (left, right, opposite_x)[kind - 6]]
        copy(there, there, (partner, tp), xw.at[0, kind], xw.at[1, kind]).wait_recv()
    for c in range(CHUNKS):
        send_rows(1, c)
    pass_rows()
    for kind in range(2):
        pool_copy(kind + 2).wait_recv()
    gates[1] = gates[1] * sum(
        jnp.dot(prow[k], w_out[1, k], preferred_element_type=f32) for k in range(4)
    )
    for c in range(CHUNKS):
        for kind in range(2):
            attn_copy(kind, 1, c).wait_recv()
            attn_copy(kind + 2, 1, c).start()

    def projected(pair, rows):
        return sum(
            jnp.dot(
                arow[pair, k, rows], w_out[0, k, pair * 128 : (pair + 1) * 128],
                preferred_element_type=f32,
            )
            for k in range(4)
        )

    for c in range(CHUNKS):
        for kind in range(2):
            attn_copy(kind + 2, 0, c).wait_recv()
    part[...] = projected(0, slice(0, ROWS))
    for c in range(CHUNKS):
        rows = slice(c * CHUNK, (c + 1) * CHUNK)
        for kind in range(2):
            attn_copy(kind + 2, 1, c).wait_recv()
        out[rows, :] = (
            gates[0, rows] * (part[rows] + projected(1, rows)) + gates[1, rows]
        ).astype(bf)

    for c in range(CHUNKS):
        for kind in range(4):
            for p in OF_CHUNK[c]:
                token_copy(kind, p).wait_send()
            for pair in range(2):
                attn_copy(kind, pair, c).wait_send()
        own_across(c).wait_send()
        for half in range(2):
            for d in range(2):
                own_first(half, d, c).wait_send()
                own_second(half, d, c).wait_send()
    for kind in range(4):
        pool_copy(kind).wait_send()
    for kind in range(9):
        weight_copy(kind).wait_send()
    for half in range(2):
        halo_copy(half).wait_send()
        for d in range(2):
            first_part(half, d).wait_send()
            for along in range(4):
                if along:
                    second_full(half, along, d).wait_send()
                second_part(half, along, d).wait_send()
        for off in ORDER[1:]:
            across_chip(half, off).wait_send()


def body(
    tokens, norm_gain, w_query_down, query_gain, w_query_up, w_latent_down, latent_gain,
    w_rotary_key, w_latent_up, query_head_gain, key_head_gain, w_pool_in, w_pool_mix, pool_scale,
    w_attn_out, w_pool_out, w_gate_attn, w_gate_pool,
):
    fine, coarse = rope_tables()

    def row(v):
        return v.reshape(1, -1)

    args = (
        tokens, row(norm_gain), w_query_down, row(query_gain), w_query_up, w_latent_down,
        row(latent_gain), w_rotary_key.T, w_latent_up, row(query_head_gain), row(key_head_gain),
        w_pool_in, w_pool_mix, row(pool_scale), w_attn_out, w_pool_out, w_gate_attn, w_gate_pool,
        fine, coarse,
    )
    dma = pltpu.SemaphoreType.DMA
    sems = [dma((17,)), dma((3,)), dma((2,)), dma((2, 4, 4)), dma((2, 4, 6)), dma((2, 4, 1))]
    sems += [dma((2, 9)), dma((2, 2)), dma((3,)), dma((3,))]
    for shape in ((2, 2, 3), (2, 2), (2, 2, 3), (2, 4, 2), (2, 4, 2), (2, 16)):
        sems += [dma(shape), dma(shape)]
    return pl.pallas_call(
        mixer_kernel,
        out_shape=pltpu.VMEM((ROWS, 512), bf),
        in_specs=[pl.BlockSpec(memory_space=pl.ANY)] * len(args),
        out_specs=pl.BlockSpec(memory_space=pltpu.VMEM),
        scratch_shapes=[
            pltpu.VMEM((4, ROWS, 512), bf),
            pltpu.VMEM((1, 2048), f32),
            pltpu.VMEM((2048, 512), bf),
            pltpu.VMEM((1, 512), f32),
            pltpu.VMEM((512, 384), bf),
            pltpu.VMEM((2048, 256), bf),
            pltpu.VMEM((1, 256), f32),
            pltpu.VMEM((32, 2048), bf),
            pltpu.VMEM((256, 512), bf),
            pltpu.VMEM((1, 96), f32),
            pltpu.VMEM((1, 96), f32),
            pltpu.VMEM((2048, 256), bf),
            pltpu.VMEM((1, 256, 256), bf),
            pltpu.VMEM((1, 256), f32),
            pltpu.VMEM((2, 2048, 512), bf),
            pltpu.VMEM((2, 16, ROWS), f32),
            pltpu.VMEM((2, 16, 128), f32),
            pltpu.VMEM((ROWS, 2048), bf),
            pltpu.VMEM((KEY_ROWS, ROWS), bf),
            pltpu.VMEM((HEADS_HERE, ROWS, 128), bf),
            pltpu.VMEM((ROWS + 32, 256), bf),
            pltpu.VMEM((16, KEY_ROWS, 2 * ROWS), bf),
            pltpu.VMEM((HEADS_HERE, ROWS, 128), f32),
            pltpu.VMEM((HEADS_HERE, 128, 2 * ROWS), bf),
            pltpu.VMEM((HEADS_HERE, 128, 2 * ROWS), bf),
            pltpu.VMEM((HEADS_HERE, 128, 2 * ROWS), bf),
            pltpu.VMEM((HEADS_HERE, 128, 2 * ROWS), bf),
            pltpu.VMEM((HEADS_HERE, 128, LATENT), bf),
            pltpu.VMEM((2, ROWS, 512), f32),
            pltpu.VMEM((ROWS, 512), f32),
            pltpu.VMEM((2, 4, 256, 512), bf),
            pltpu.VMEM((2, 128, 512), bf),
            pltpu.VMEM((4, ROWS, 256), bf),
            pltpu.VMEM((2, 4, ROWS, 128), bf),
        ]
        + sems,
        compiler_params=pltpu.CompilerParams(
            collective_id=0, has_side_effects=True, vmem_limit_bytes=60 * 2**20
        ),
        name="mixer",
    )(*args)


def solution(mesh):
    placed = (
        P("sp", "tp"), P(), P(), P(), P(None, "tp"), P(), P(), P(), P(None, "tp"), P(), P(),
        P(None, "tp"), P("tp", None, None), P("tp"), P("tp", None), P("tp", None),
        P(None, "tp"), P(None, "tp"),
    )
    return jax.shard_map(body, mesh=mesh, in_specs=placed, out_specs=P("sp", "tp"), check_vma=False)
```
